32 devices in a mesh: sp: 16 (over z, y, x), tp: 2 (over core).
Axes of the slice: x: 2, y: 2, z: 4, core: 2. Of those that a mesh axis runs over, the one named last changes fastest.
Arguments:
- block_input: bfloat16 [2048, 2048], P('sp'), may hold values from -6 to 6
- value_weight: bfloat16 [2048, 384], P(None, 'tp'), may hold values from -0.125 to 0.125
- query_pre: bfloat16 [2048, 384], P('sp', 'tp'), may hold values from -6 to 6
- forget_pre: bfloat16 [2048, 384], P('sp', 'tp'), may hold values from -5.5 to 5.5
- lower_bound: float32 [384], P('tp'), may hold values from 0.94 to 1, as said below
- out_grad: bfloat16 [2048, 384], P('sp', 'tp'), may hold values from -6 to 6
Outputs:
- grad_query_pre: bfloat16 [2048, 384], P('sp', 'tp')
- grad_forget_pre: bfloat16 [2048, 384], P('sp', 'tp')
- grad_block_input: bfloat16 [2048, 2048], P(('sp', 'tp'))
- grad_value_weight: float32 [2048, 384], P('sp', 'tp')
The draws below stay inside these ranges and needn't reach their ends.
Inputs may be any that keep to these rules, and one draw needn't show every extreme that they name: `lower_bound`: each channel's floor is below 1 and at least 0.94.
All inputs are finite; a program needn't handle non-finite values.
Results may differ from the reference program's by a relative error of at most 0.009.
Values may be sent and summed in bfloat16 or wider, within the bound.
A program may use at most 64 MiB of HBM per device.

```python
import math
import jax
import jax.numpy as jnp
from jax import lax

D = 2048
HEADS = 6
HEAD = 64
BLOCK = 64
TOK_DEV = 128
WIDTH = 384
TOKENS = 2048
N_TP = 2


def draw_lower_bound(key, part):
    pick_key, fast_key, slow_key = jax.random.split(jax.random.fold_in(key, 11), 3)
    fast_share = 0.5
    head_fast = jax.random.uniform(pick_key, (HEADS,), jnp.float32) < fast_share
    channel_fast = jnp.repeat(head_fast, HEAD)
    fast_gap = jnp.exp(jax.random.uniform(fast_key, (WIDTH,), jnp.float32, math.log(0.02), math.log(0.06)))
    slow_gap = 2.0 / TOKENS * jnp.exp(jax.random.uniform(slow_key, (WIDTH,), jnp.float32, math.log(0.5), math.log(2.0)))
    return (1.0 - jnp.where(channel_fast, fast_gap, slow_gap)).astype(jnp.float32)


def draw_forget_pre(key, part):
    noise_key, shift_key = jax.random.split(jax.random.fold_in(key, 23), 2)
    noise = jnp.clip(jax.random.normal(noise_key, (TOKENS, WIDTH), jnp.float32), -4.0, 4.0)
    shifts = jax.random.uniform(shift_key, (TOKENS // TOK_DEV, WIDTH), jnp.float32, -1.5, 1.5)
    return (noise + jnp.repeat(shifts, TOK_DEV, axis=0)).astype(jnp.bfloat16)


def steps_of(stream_key, shape, shards, low, top_value):
    factor_of, own = 1.0, jax.random.fold_in(stream_key, 6)
    for axis_at, shards_of in shards:
        draws = jnp.exp(jax.random.uniform(jax.random.fold_in(own, axis_at), (shards_of,), jnp.float32, low / len(shards), top_value / len(shards)))
        factor_of = factor_of * jnp.repeat(draws, shape[axis_at] // shards_of).reshape([-1 if axis == axis_at else 1 for axis in range(len(shape))])
    return factor_of


def gaussian(own_key, shape, spread, bound, cuts=(), held_as=jnp.bfloat16):
    loudness = steps_of(own_key, shape, cuts, -0.22, 0.18) if cuts else 1.0
    values = jax.random.normal(own_key, shape, jnp.float32) * spread * loudness
    return jnp.minimum(jnp.maximum(values, -bound), bound).astype(held_as)


def setup_inputs(seed: int = 0) -> dict:
    key_list = jax.random.split(jax.random.key(seed), 7)
    return {
        "block_input": gaussian(key_list[0], (TOKENS, D), 1.0, 6.0, ((0, 16),)),
        "value_weight": gaussian(key_list[1], (D, WIDTH), D ** -0.5, 0.125, ((1, 2),)),
        "query_pre": gaussian(key_list[2], (TOKENS, WIDTH), 1.0, 6.0, ((0, 16), (1, 2))),
        "forget_pre": draw_forget_pre(jax.random.fold_in(key_list[6], 71), 0),
        "lower_bound": draw_lower_bound(jax.random.fold_in(key_list[6], 71), 0),
        "out_grad": gaussian(key_list[5], (TOKENS, WIDTH), 1.0, 6.0, ((0, 16), (1, 2))),
    }


highest = lax.Precision.HIGHEST

def blocked(array, head_count, block_count):
    return jnp.transpose(array.reshape(block_count, BLOCK, head_count, HEAD), (0, 2, 1, 3))

def recurrence(query, key_rate, value_rows, decay_log):
    tokens_all, width_all = query.shape
    head_count = width_all // HEAD
    block_count = tokens_all // BLOCK
    causal = (jnp.arange(BLOCK)[:, None] >= jnp.arange(BLOCK)[None, :]).astype(query.dtype)

    def advance(carried, pieces):
        query_b, key_b, value_b, decay_b = pieces
        cumulative = jnp.cumsum(decay_b, axis=1)
        closing = cumulative[:, -1:, :]
        query_dec = query_b * jnp.exp(cumulative)
        key_dec = key_b * jnp.exp(-cumulative)
        mixing = jnp.einsum('htd,hsd->hts', query_dec, key_dec, precision=highest) * causal
        output = jnp.einsum('hts,hsv->htv', mixing, value_b, precision=highest)
        output = output + jnp.einsum('htd,hdv->htv', query_dec, carried, precision=highest)
        renewed = jnp.exp(closing[:, 0, :])[:, :, None] * carried
        renewed = renewed + jnp.einsum('hsd,hsv->hdv', key_b * jnp.exp(closing - cumulative), value_b, precision=highest)
        return (renewed, output)
    initial = jnp.zeros((head_count, HEAD, HEAD), query.dtype)
    pieces = tuple((blocked(array, head_count, block_count) for array in (query, key_rate, value_rows, decay_log)))
    _, outputs = lax.scan(advance, initial, pieces)
    return jnp.transpose(outputs, (0, 2, 1, 3)).reshape(tokens_all, width_all)

def reference(block_input, value_weight, query_pre, forget_pre, lower_bound, out_grad):
    value_rows = jnp.dot(block_input, value_weight, preferred_element_type=jnp.float32).astype(jnp.bfloat16)

    def forward(query_f, forget_f, value_f):
        query = jax.nn.silu(query_f)
        key_rate = (1.0 - lower_bound) * jax.nn.sigmoid(-forget_f)
        decay_log = jnp.log1p(-key_rate)
        return recurrence(query, key_rate, value_f, decay_log)
    _, pullback = jax.vjp(forward, query_pre.astype(jnp.float32), forget_pre.astype(jnp.float32), value_rows.astype(jnp.float32))
    grad_query, grad_forget, grad_value = pullback(out_grad.astype(jnp.float32))
    value_grad = grad_value.astype(jnp.bfloat16)
    weight_grad = lax.dot_general(block_input, value_grad, (((0,), (0,)), ((), ())), preferred_element_type=jnp.float32)
    group_width = WIDTH // N_TP
    summed = jnp.zeros((block_input.shape[0], D), jnp.float32)
    for member in range(N_TP):
        lo_col = member * group_width
        partial_value = lax.dot_general(value_grad[:, lo_col:lo_col + group_width], value_weight[:, lo_col:lo_col + group_width], (((1,), (1,)), ((), ())), preferred_element_type=jnp.float32)
        partial_value = lax.optimization_barrier(partial_value.astype(jnp.bfloat16))
        summed = summed + partial_value.astype(jnp.float32)
    return (grad_query.astype(jnp.bfloat16), grad_forget.astype(jnp.bfloat16), summed.astype(jnp.bfloat16), weight_grad)
```

```python
import functools

import jax
import jax.numpy as jnp
from jax import lax
from jax.experimental import pallas as pl
from jax.experimental.pallas import tpu as pltpu
from jax.sharding import PartitionSpec as P

HEAD = 64
MESH = pl.DeviceIdType.MESH
f32, bf16 = jnp.float32, jnp.bfloat16
LOGROWS = 16


def nn(a, b):
    return lax.dot_general(a, b, (((1,), (0,)), ((), ())), preferred_element_type=f32)


def nt(a, b):
    return lax.dot_general(a, b, (((1,), (1,)), ((), ())), preferred_element_type=f32)


def tn(a, b):
    return lax.dot_general(a, b, (((0,), (0,)), ((), ())), preferred_element_type=f32)


def split(a):
    high = a.astype(bf16)
    return high, (a - high.astype(f32)).astype(bf16)


def kernel(
    n, n_tp, part,
    x_ref, w_ref, q_ref, f_ref, lb_ref, g_ref,
    gq_ref, gf_ref, gx_ref, gw_ref,
    w_all, xt, xg, smsg, sbuf, dvg, dvp,
    w_send, w_recv, x_send, x_recv, r_send, r_recv, s_send, s_recv,
    d_send, d_recv, p_send, p_recv,
):
    me, core = lax.axis_index("sp"), lax.axis_index("tp")
    tokens, depth = x_ref.shape
    width = q_ref.shape[1]
    heads = width // HEAD
    rows = depth // n
    piece = rows // part
    half = tokens // n_tp

    barrier = pltpu.get_barrier_semaphore()
    for k in range(1, n):
        pl.semaphore_signal(
            barrier, inc=1, device_id=(lax.rem(me + k, n), core), device_id_type=MESH
        )
    for k in range(1, n_tp):
        pl.semaphore_signal(
            barrier, inc=1, device_id=(me, lax.rem(core + k, n_tp)), device_id_type=MESH
        )
    pl.semaphore_wait(barrier, n - 1 + n_tp - 1)

    def mate(k):
        return (me, lax.rem(core + k, n_tp))

    def peer(k):
        return (lax.rem(me + k, n), core)

    def copy_w(k):
        return pltpu.make_async_remote_copy(
            w_ref, w_all.at[k - 1], w_send.at[k - 1], w_recv.at[k - 1], mate(k), MESH
        )

    lead = core * (part - 1)

    def copy_x(k):
        start = pl.multiple_of(lax.rem(me + k, n) * rows + lead * piece, piece)
        lanes = pl.ds(pl.multiple_of(me * tokens, tokens), tokens)
        return pltpu.make_async_remote_copy(
            xt.at[pl.ds(start, piece), :],
            xg.at[lead, :, lanes],
            x_send.at[k - 1], x_recv.at[k - 1], peer(k), MESH,
        )

    def copy_r():
        return pltpu.make_async_remote_copy(
            xg.at[lead], xg.at[lead], r_send.at[0], r_recv.at[0], mate(1), MESH
        )

    def copy_s(k, src):
        return pltpu.make_async_remote_copy(
            smsg.at[(me + k) // n], sbuf.at[src], s_send.at[k - 1], s_recv.at[k - 1], peer(k), MESH
        )

    def copy_d(k):
        mine = dvg.at[pl.ds(pl.multiple_of(me * tokens, tokens), tokens), :]
        return pltpu.make_async_remote_copy(
            mine, mine, d_send.at[k - 1], d_recv.at[k - 1], peer(k), MESH
        )

    def copy_p(k):
        other = lax.rem(core + k, n_tp)
        start = pl.multiple_of(me * tokens + other * half, half)
        return pltpu.make_async_remote_copy(
            dvg.at[pl.ds(start, half), :], dvp.at[k - 1],
            p_send.at[k - 1], p_recv.at[k - 1], mate(k), MESH,
        )

    t_at = lax.broadcasted_iota(jnp.int32, (tokens, tokens), 0)
    s_at = lax.broadcasted_iota(jnp.int32, (tokens, tokens), 1)
    lower = t_at >= s_at
    upper = t_at <= s_at
    lower_b = lower.astype(f32).astype(bf16)
    upper_b = upper.astype(f32).astype(bf16)
    lane_head = lax.broadcasted_iota(jnp.int32, (1, width), 1) // HEAD
    masks = [(lane_head == h).astype(f32) for h in range(heads)]
    masks_b = [m.astype(bf16) for m in masks]

    def stacked(a):
        return jnp.concatenate([a * m for m in masks_b], axis=0)

    def diagonal(full):
        return sum(full[h * HEAD : (h + 1) * HEAD, :] * masks[h] for h in range(heads))

    q_in = q_ref[...].astype(f32)
    f_in = f_ref[...].astype(f32)
    lb = lb_ref[...]
    q_sig = jax.nn.sigmoid(q_in)
    query = q_in * q_sig
    f_sig = jax.nn.sigmoid(f_in)
    key = (1.0 - lb) * jax.nn.sigmoid(-f_in)
    high, low = split(jnp.log1p(-key))
    cumulative = nn(lower_b, high) + nn(lower_b, low)
    closing = cumulative[tokens - 1 : tokens, :]
    growth = jnp.exp(cumulative)
    shrinking = jnp.exp(-cumulative)
    remaining = jnp.exp(closing - cumulative)
    q_dec = (query * growth).astype(bf16)
    k_dec = (key * shrinking).astype(bf16)
    k_end = (key * remaining).astype(bf16)
    g = g_ref[...]
    reach = diagonal(tn(g, q_dec))
    value = nn(x_ref[...], w_ref[...]).astype(bf16)
    update = diagonal(tn(value, k_end))
    log_high, log_low = split(closing)
    row_at = lax.broadcasted_iota(jnp.int32, (LOGROWS, width), 0)
    logs = jnp.where(row_at == 0, log_high.astype(f32), log_low.astype(f32)).astype(bf16)
    for way, part_state in ((0, update), (1, reach)):
        smsg[way, 0:HEAD, :] = part_state.astype(bf16)
        smsg[way, HEAD : HEAD + LOGROWS, :] = logs
    for k in range(1, n):
        copy_s(k, me).start()
    for k in range(1, n_tp):
        copy_w(k).start()
    xt[...] = x_ref[...].T
    for k in range(1, n):
        copy_x(k).start()
    start = pl.multiple_of(me * rows + lead * piece, piece)
    xg[lead, :, pl.ds(pl.multiple_of(me * tokens, tokens), tokens)] = xt[pl.ds(start, piece), :]

    g3, q3, k3, v3 = stacked(g), stacked(q_dec), stacked(k_dec), stacked(value)
    upper3 = jnp.concatenate([upper] * heads, axis=1)
    lower3 = jnp.concatenate([lower] * heads, axis=1)
    mixing_t = jnp.where(upper3, nt(k_dec, q3), 0.0).astype(bf16)
    gv_local = nn(mixing_t, g3)
    pairing_t = jnp.where(upper3, nt(value, g3), 0.0).astype(bf16)
    gk_local = nn(pairing_t, q3)
    pairing = jnp.where(lower3, nt(g, v3), 0.0).astype(bf16)
    gq_local = nn(pairing, k3)

    empty = jnp.zeros((HEAD, width), f32)
    none = jnp.zeros((1, width), f32)

    def take(b, k, carried):
        total, weight_log = carried
        copy_s(k, b).wait_recv()
        total = total + jnp.exp(weight_log) * sbuf[b, 0:HEAD, :].astype(f32)
        tail = sbuf[b, HEAD : HEAD + LOGROWS, :].astype(f32)
        return total, weight_log + tail[0:1, :] + tail[1:2, :]

    outgoing, _ = lax.fori_loop(
        0, n - 1 - me, lambda i, c: take(me + 1 + i, n - 1 - i, c), (empty, none)
    )
    out_b = stacked(outgoing.astype(bf16))
    grad_value = gv_local + nt(k_end, out_b)
    value_grad = grad_value.astype(bf16)
    own = pl.ds(pl.multiple_of(me * tokens, tokens), tokens)
    dvg[own, :] = value_grad
    for k in range(1, n_tp):
        copy_p(k).start()
    for k in range(1, n):
        copy_d(k).start()
    incoming, _ = lax.fori_loop(0, me, lambda i, c: take(me - 1 - i, i + 1, c), (empty, none))

    in_b = stacked(incoming.astype(bf16))
    grad_query = growth * (gq_local + nn(g, in_b))
    grad_key = shrinking * gk_local + remaining * nn(value, out_b)
    ends = jnp.exp(closing) * incoming + update
    boundary = jnp.sum(outgoing * ends, axis=0, keepdims=True)
    c_high, c_low = split(query * grad_query - key * grad_key)
    grad_decay = nn(upper_b, c_high) + nn(upper_b, c_low) + boundary
    gq_ref[...] = (grad_query * (q_sig * (1.0 + q_in * (1.0 - q_sig)))).astype(bf16)
    gf_ref[...] = (-(grad_key - grad_decay / (1.0 - key)) * key * f_sig).astype(bf16)

    for k in range(1, n):
        copy_x(k).wait_recv()
    if part > 1:
        copy_r().start()

    half_rows = pl.ds(pl.multiple_of(me * tokens + core * half, half), half)
    gx = nt(dvg[half_rows, :], w_ref[...]).astype(bf16).astype(f32)
    for k in range(1, n_tp):
        copy_w(k).wait_recv()
        copy_p(k).wait_recv()
        gx = gx + nt(dvp[k - 1], w_all[k - 1]).astype(bf16).astype(f32)
    gx_ref[...] = gx.astype(bf16)

    if part > 1:
        pltpu.make_async_remote_copy(
            xg.at[1 - lead], xg.at[1 - lead], r_send.at[0], r_recv.at[0], mate(1), MESH
        ).wait_recv()
    for k in range(1, n):
        pltpu.make_async_remote_copy(
            dvg.at[own, :],
            dvg.at[pl.ds(pl.multiple_of(lax.rem(me + n - k, n) * tokens, tokens), tokens), :],
            d_send.at[k - 1], d_recv.at[k - 1], peer(k), MESH,
        ).wait_recv()
    for p in range(part):
        gw_ref[pl.ds(p * piece, piece), :] = nn(xg[p], dvg[...])

    for k in range(1, n_tp):
        copy_w(k).wait_send()
        copy_p(k).wait_send()
    if part > 1:
        copy_r().wait_send()
    for k in range(1, n):
        copy_s(k, me).wait_send()
        copy_x(k).wait_send()
        copy_d(k).wait_send()


def on_device(n, n_tp, block_input, value_weight, query_pre, forget_pre, lower_bound, out_grad):
    tokens, depth = block_input.shape
    width = query_pre.shape[1]
    rows = depth // n
    part = 2 if n_tp == 2 and rows % 32 == 0 else 1
    dma = pltpu.SemaphoreType.DMA
    vmem = pl.BlockSpec(memory_space=pltpu.VMEM)
    return pl.pallas_call(
        functools.partial(kernel, n, n_tp, part),
        out_shape=(
            jax.ShapeDtypeStruct((tokens, width), bf16),
            jax.ShapeDtypeStruct((tokens, width), bf16),
            jax.ShapeDtypeStruct((tokens // n_tp, depth), bf16),
            jax.ShapeDtypeStruct((rows, width), f32),
        ),
        in_specs=[vmem] * 6,
        out_specs=(vmem,) * 4,
        scratch_shapes=[
            pltpu.VMEM((n_tp - 1, depth, width), bf16),
            pltpu.VMEM((depth, tokens), bf16),
            pltpu.VMEM((part, rows // part, n * tokens), bf16),
            pltpu.VMEM((2, HEAD + LOGROWS, width), bf16),
            pltpu.VMEM((n, HEAD + LOGROWS, width), bf16),
            pltpu.VMEM((n * tokens, width), bf16),
            pltpu.VMEM((n_tp - 1, tokens // n_tp, width), bf16),
            dma((n_tp - 1,)), dma((n_tp - 1,)),
            dma((n - 1,)), dma((n - 1,)),
            dma((1,)), dma((1,)),
            dma((n - 1,)), dma((n - 1,)),
            dma((n - 1,)), dma((n - 1,)),
            dma((n_tp - 1,)), dma((n_tp - 1,)),
        ],
        compiler_params=pltpu.CompilerParams(
            collective_id=0, has_side_effects=True, vmem_limit_bytes=60 * 1024 * 1024
        ),
    )(block_input, value_weight, query_pre, forget_pre, lower_bound[None, :], out_grad)


def solution(mesh):
    n, n_tp = mesh.shape["sp"], mesh.shape["tp"]
    in_specs = (P("sp", None), P(None, "tp"), P("sp", "tp"), P("sp", "tp"), P("tp"), P("sp", "tp"))
    out_specs = (P("sp", "tp"), P("sp", "tp"), P(("sp", "tp"), None), P("sp", "tp"))
    return jax.shard_map(
        functools.partial(on_device, n, n_tp),
        mesh=mesh, in_specs=in_specs, out_specs=out_specs, check_vma=False,
    )
```

```python
import functools

import jax
import jax.numpy as jnp
from jax import lax
from jax.experimental import pallas as pl
from jax.experimental.pallas import tpu as pltpu
from jax.sharding import PartitionSpec as P

HEAD = 64
MESH = pl.DeviceIdType.MESH
f32, bf16 = jnp.float32, jnp.bfloat16
LOGROWS = 16


def nn(a, b):
    return lax.dot_general(a, b, (((1,), (0,)), ((), ())), preferred_element_type=f32)


def nt(a, b):
    return lax.dot_general(a, b, (((1,), (1,)), ((), ())), preferred_element_type=f32)


def tn(a, b):
    return lax.dot_general(a, b, (((0,), (0,)), ((), ())), preferred_element_type=f32)


def split(a):
    high = a.astype(bf16)
    return high, (a - high.astype(f32)).astype(bf16)


def kernel(
    inner, outer, n_tp, part,
    x_ref, w_ref, q_ref, f_ref, lb_ref, g_ref,
    gq_ref, gf_ref, gx_ref, gw_ref,
    w_all, xt, xg, b1, f1, bmsg, fmsg, b2, f2, gvk, dvp, dvm, pmsg, pin, dvs,
    w_send, w_recv, x_send, x_recv, r_send, r_recv, b1_send, b1_recv, f1_send, f1_recv,
    b2_send, b2_recv, f2_send, f2_recv, k_send, k_recv, m_send, m_recv, p_send, p_recv,
):
    me, core = lax.axis_index("sp"), lax.axis_index("tp")
    here, plane = lax.rem(me, inner), me // inner
    tokens, depth = x_ref.shape
    width = q_ref.shape[0]
    heads = width // HEAD
    half = tokens // n_tp
    pairs, odd = heads // 2, heads % 2
    wide = 2 * HEAD
    packed = pairs * HEAD + odd * HEAD // 2

    def near(k):
        return (plane * inner + lax.rem(here + k, inner), core)

    def column(k):
        return (lax.rem(plane + k, outer) * inner + here, core)

    def mate(k):
        return (me, lax.rem(core + k, n_tp))

    def rc(src, dst, send, recv, k, to):
        return pltpu.make_async_remote_copy(src, dst, send.at[k - 1], recv.at[k - 1], to, MESH)

    barrier = pltpu.get_barrier_semaphore()
    for to, count in ((near, inner), (column, outer), (mate, n_tp)):
        for k in range(1, count):
            pl.semaphore_signal(barrier, inc=1, device_id=to(k), device_id_type=MESH)

    lead = core * (part - 1)
    own_lanes = pl.ds(pl.multiple_of(here * tokens, tokens), tokens)

    def copy_w(k):
        return rc(w_ref, w_all.at[k - 1], w_send, w_recv, k, mate(k))

    def copy_x(k):
        return rc(
            xt.at[:, lax.rem(here + k, inner), lead], xg.at[:, lead, :, own_lanes],
            x_send, x_recv, k, near(k),
        )

    def copy_r(lane):
        return rc(xg.at[:, lane], xg.at[:, lane], r_send, r_recv, 1, mate(1))

    def copy_b1(k, at):
        return rc(b1.at[at], b1.at[at], b1_send, b1_recv, k, near(k))

    def copy_f1(k, at):
        return rc(f1.at[at], f1.at[at], f1_send, f1_recv, k, near(k))

    def copy_k(k, at):
        return rc(gvk.at[at], gvk.at[at], k_send, k_recv, k, near(k))

    def copy_b2(k, at):
        return rc(bmsg, b2.at[at], b2_send, b2_recv, k, column(k))

    def copy_f2(k, at):
        return rc(fmsg, f2.at[at], f2_send, f2_recv, k, column(k))

    def copy_m(k):
        return rc(dvp.at[:, own_lanes], dvm.at[k - 1], m_send, m_recv, k, mate(k))

    def copy_p(k):
        return rc(pmsg.at[lax.rem(plane + k, outer)], pin.at[k - 1], p_send, p_recv, k, column(k))

    def source(k):
        return lax.rem(here + inner - k, inner)

    lane_low = lax.broadcasted_iota(jnp.int32, (1, wide), 1) < HEAD

    def pairs_of(a, j):
        return a[j * wide : (j + 1) * wide, :]

    def twice(a):
        return jnp.concatenate([a[pairs * wide :, :]] * 2, axis=0)

    def pack(values, keys):
        out = []
        for j in range(pairs):
            full = nt(pairs_of(values, j), pairs_of(keys, j))
            out.append(jnp.where(lane_low, full[:HEAD, :], full[HEAD:, :]))
        if odd:
            full = nt(values[pairs * wide :, :], twice(keys))
            out.append(jnp.where(lane_low, full[: HEAD // 2, :], full[HEAD // 2 :, :]))
        return jnp.concatenate(out, axis=0)

    def opened(state):
        out = []
        for j in range(pairs + odd):
            size = HEAD if j < pairs else HEAD // 2
            rows_of = state[j * HEAD : j * HEAD + size, :]
            out.append(
                jnp.concatenate(
                    [jnp.where(lane_low, rows_of, 0.0), jnp.where(lane_low, 0.0, rows_of)], axis=0
                ).astype(bf16)
            )
        return out

    def from_keys(blocks, a):
        out = [nn(blocks[j], pairs_of(a, j)) for j in range(pairs)]
        if odd:
            out.append(nn(blocks[pairs], twice(a)))
        return jnp.concatenate(out, axis=0)

    def from_values(blocks, a):
        out = [tn(blocks[j], pairs_of(a, j)) for j in range(pairs)]
        if odd:
            full = tn(blocks[pairs], a[pairs * wide :, :])
            out.append(full[:HEAD, :] + full[HEAD:, :])
        return jnp.concatenate(out, axis=0)

    def scaled(logs, state):
        out = []
        for j in range(pairs + odd):
            size = HEAD if j < pairs else HEAD // 2
            out.append(jnp.exp(logs[j]) * state[j * HEAD : j * HEAD + size, :])
        return jnp.concatenate(out, axis=0)

    row_at = lax.broadcasted_iota(jnp.int32, (LOGROWS, wide), 0)

    def log_rows(logs):
        rows_f = jnp.zeros((LOGROWS, wide), f32)
        for j, log in enumerate(logs):
            high, low = split(log)
            rows_f = jnp.where(row_at == 2 * j, high.astype(f32), rows_f)
            rows_f = jnp.where(row_at == 2 * j + 1, low.astype(f32), rows_f)
        return rows_f.astype(bf16)

    def read(ref, at):
        state = ref[at, 0:packed, :].astype(f32)
        tail = ref[at, packed : packed + LOGROWS, :].astype(f32)
        logs = [tail[2 * j : 2 * j + 1, :] + tail[2 * j + 1 : 2 * j + 2, :] for j in range(pairs + odd)]
        return state, logs

    def added(a, b):
        return [p + q for p, q in zip(a, b)]

    s_at = lax.broadcasted_iota(jnp.int32, (tokens, tokens), 0)
    t_at = lax.broadcasted_iota(jnp.int32, (tokens, tokens), 1)
    upper, lower = s_at <= t_at, s_at >= t_at
    upper_b, lower_b = upper.astype(f32).astype(bf16), lower.astype(f32).astype(bf16)
    ones = jnp.ones((LOGROWS, tokens), bf16)
    lb = jnp.broadcast_to(lb_ref[...], (tokens, width)).T
    f_in = f_ref[...].astype(f32)
    f_sig = jax.nn.sigmoid(f_in)
    key = (1.0 - lb) * jax.nn.sigmoid(-f_in)
    high, low = split(jnp.log1p(-key))
    cumulative = nn(high, upper_b) + nn(low, upper_b)
    growth = jnp.exp(cumulative)
    q_in = q_ref[...].astype(f32)
    q_sig = jax.nn.sigmoid(q_in)
    query = q_in * q_sig
    q_dec = (query * growth).astype(bf16)
    g = g_ref[...]
    logs = []
    for j in range(pairs):
        logs.append((nt(ones, pairs_of(high, j)) + nt(ones, pairs_of(low, j)))[0:1, :])
    if odd:
        logs.append((nt(ones, twice(high)) + nt(ones, twice(low)))[0:1, :])
    tail = log_rows(logs)
    b1[here, 0:packed, :] = pack(g, q_dec).astype(bf16)
    b1[here, packed : packed + LOGROWS, :] = tail
    pl.semaphore_wait(barrier, inner + outer + n_tp - 3)
    for k in range(1, inner):
        copy_b1(k, here).start()
    for k in range(1, n_tp):
        copy_w(k).start()

    value = nt(w_ref[...], x_ref[...]).astype(bf16)
    closing = cumulative[:, tokens - 1 : tokens]
    k_end = (key * jnp.exp(closing - cumulative)).astype(bf16)
    update = pack(value, k_end)
    f1[here, 0:packed, :] = update.astype(bf16)
    f1[here, packed : packed + LOGROWS, :] = tail
    for k in range(1, inner):
        copy_f1(k, here).start()
    shrinking = jnp.exp(-cumulative)
    k_dec = (key * shrinking).astype(bf16)

    def of(a, h):
        return a[h * HEAD : (h + 1) * HEAD, :]

    mixing = [jnp.where(upper, tn(of(k_dec, h), of(q_dec, h)), 0.0).astype(bf16) for h in range(heads)]
    gv_local = jnp.concatenate([nt(of(g, h), mixing[h]) for h in range(heads)], axis=0)
    gvk[here, 0] = gv_local.astype(bf16)
    gvk[here, 1] = k_end
    for k in range(1, inner):
        copy_k(k, here).start()
    xt[...] = x_ref[...].T.reshape(xt.shape)
    for k in range(1, inner):
        copy_x(k).start()
    xg[:, lead, :, own_lanes] = xt[:, here, lead]

    for k in range(1, inner):
        copy_b1(k, source(k)).wait_recv()
    inside, after = [None] * inner, [None] * inner
    running = jnp.zeros((packed, wide), f32)
    plane_logs = [jnp.zeros((1, wide), f32) for _ in range(pairs + odd)]
    for j in reversed(range(inner)):
        inside[j], after[j] = running, plane_logs
        state, own_logs = read(b1, j)
        running = state + scaled(own_logs, running)
        plane_logs = added(plane_logs, own_logs)
    plane_tail = log_rows(plane_logs)
    bmsg[0:packed, :] = running.astype(bf16)
    bmsg[packed : packed + LOGROWS, :] = plane_tail

    def each(lo, hi, act):
        def step(i, carried):
            act(i)
            return carried

        lax.fori_loop(lo, hi, step, 0)

    each(outer - plane, outer, lambda k: copy_b2(k, plane).start())

    for k in range(1, inner):
        copy_f1(k, source(k)).wait_recv()
    running = jnp.zeros((packed, wide), f32)
    before = [jnp.zeros((1, wide), f32) for _ in range(pairs + odd)]
    incoming = running
    in_logs = before
    for j in range(inner):
        incoming = jnp.where(here == j, running, incoming)
        in_logs = [jnp.where(here == j, p, q) for p, q in zip(before, in_logs)]
        state, own_logs = read(f1, j)
        running = state + scaled(own_logs, running)
        before = added(before, own_logs)
    fmsg[0:packed, :] = running.astype(bf16)
    fmsg[packed : packed + LOGROWS, :] = plane_tail
    each(1, outer - plane, lambda k: copy_f2(k, plane).start())

    pairing = [jnp.where(upper, tn(of(value, h), of(g, h)), 0.0).astype(bf16) for h in range(heads)]
    gk_local = jnp.concatenate([nt(of(q_dec, h), pairing[h]) for h in range(heads)], axis=0)
    gq_local = jnp.concatenate([nn(of(k_dec, h), pairing[h]) for h in range(heads)], axis=0)

    for k in range(1, inner):
        lanes = pl.ds(pl.multiple_of(source(k) * tokens, tokens), tokens)
        rc(xt.at[:, 0, lead], xg.at[:, lead, :, lanes], x_send, x_recv, k, near(k)).wait_recv()
    if part > 1:
        copy_r(lead).start()

    empty = jnp.zeros((packed, wide), f32)
    none = [jnp.zeros((1, wide), f32) for _ in range(pairs + odd)]

    def entering(ref, copy, count, place, distance):
        def step(i, carried):
            total, weight = carried
            copy(distance(i), place(i)).wait_recv()
            state, own_logs = read(ref, place(i))
            return total + scaled(weight, state), added(weight, own_logs)

        return lax.fori_loop(0, count, step, (empty, none))[0]

    below = entering(
        b2, copy_b2, outer - 1 - plane, lambda i: plane + 1 + i, lambda i: outer - 1 - i
    )
    outgoing = empty
    for k in range(1, inner):
        copy_k(k, source(k)).wait_recv()
    for j in range(inner):
        grad_state = inside[j] + scaled(after[j], below)
        outgoing = jnp.where(here == j, grad_state, outgoing)
        value_grad = gvk[j, 0].astype(f32) + from_keys(opened(grad_state), gvk[j, 1])
        dvp[:, j * tokens : (j + 1) * tokens] = value_grad.astype(bf16)
    for k in range(1, n_tp):
        copy_m(k).start()
    if part > 1:
        copy_r(1 - lead).wait_recv()
    for z in range(outer):
        pieces = [nt(dvp[...], xg[z, p]) for p in range(part)]
        pmsg[z] = jnp.concatenate(pieces, axis=1).astype(bf16)
    for k in range(1, outer):
        copy_p(k).start()

    def rows_half(a, slot):
        dvs[slot] = a.T
        return dvs[slot, pl.ds(pl.multiple_of(core * half, half), half), :]

    gx = nn(rows_half(dvp[:, own_lanes], 0), w_ref[...]).astype(bf16).astype(f32)
    for k in range(1, n_tp):
        copy_w(k).wait_recv()
        copy_m(k).wait_recv()
        gx = gx + nn(rows_half(dvm[k - 1], k), w_all[k - 1]).astype(bf16).astype(f32)
    gx_ref[...] = gx.astype(bf16)

    above = entering(f2, copy_f2, plane, lambda i: plane - 1 - i, lambda i: i + 1)
    incoming = incoming + scaled(in_logs, above)
    grad_query = growth * (gq_local + from_values(opened(incoming), g))
    remaining = jnp.exp(closing - cumulative)
    grad_key = shrinking * gk_local + remaining * from_values(opened(outgoing), value)
    product = outgoing * (scaled(logs, incoming) + update)
    p_high, p_low = split(product)
    bound = []
    for j in range(pairs + odd):
        size = HEAD if j < pairs else HEAD // 2
        every = jnp.ones((size, tokens), bf16)
        at = slice(j * HEAD, j * HEAD + size)
        full = tn(p_high[at, :], every) + tn(p_low[at, :], every)
        bound.append(full if j < pairs else full[:HEAD, :] + full[HEAD:, :])
    boundary = jnp.concatenate(bound, axis=0)
    c_high, c_low = split(query * grad_query - key * grad_key)
    grad_decay = nn(c_high, lower_b) + nn(c_low, lower_b) + boundary
    gq_ref[...] = (grad_query * (q_sig * (1.0 + q_in * (1.0 - q_sig)))).astype(bf16)
    gf_ref[...] = (-(grad_key - grad_decay / (1.0 - key)) * key * f_sig).astype(bf16)

    total = pmsg[plane].astype(f32)
    for k in range(1, outer):
        copy_p(k).wait_recv()
        total = total + pin[k - 1].astype(f32)
    gw_ref[...] = total

    for k in range(1, n_tp):
        copy_w(k).wait_send()
        copy_m(k).wait_send()
    if part > 1:
        copy_r(lead).wait_send()
    for k in range(1, inner):
        copy_b1(k, here).wait_send()
        copy_f1(k, here).wait_send()
        copy_k(k, here).wait_send()
        copy_x(k).wait_send()
    each(outer - plane, outer, lambda k: copy_b2(k, plane).wait_send())
    each(1, outer - plane, lambda k: copy_f2(k, plane).wait_send())
    for k in range(1, outer):
        copy_p(k).wait_send()


def on_device(n, n_tp, block_input, value_weight, query_pre, forget_pre, lower_bound, out_grad):
    tokens, depth = block_input.shape
    width = query_pre.shape[1]
    heads = width // HEAD
    rows = depth // n
    inner = 1
    while n % (inner * 2) == 0 and (inner * 2) ** 2 <= n:
        inner *= 2
    outer = n // inner
    part = 2 if n_tp == 2 and rows % 32 == 0 else 1
    message = (heads // 2) * HEAD + (heads % 2) * HEAD // 2 + LOGROWS
    dma = pltpu.SemaphoreType.DMA
    vmem = pl.BlockSpec(memory_space=pltpu.VMEM)
    gq, gf, gx, gw = pl.pallas_call(
        functools.partial(kernel, inner, outer, n_tp, part),
        out_shape=(
            jax.ShapeDtypeStruct((width, tokens), bf16),
            jax.ShapeDtypeStruct((width, tokens), bf16),
            jax.ShapeDtypeStruct((tokens // n_tp, depth), bf16),
            jax.ShapeDtypeStruct((width, rows), f32),
        ),
        in_specs=[vmem] * 6,
        out_specs=(vmem,) * 4,
        scratch_shapes=[
            pltpu.VMEM((n_tp - 1, width, depth), bf16),
            pltpu.VMEM((outer, inner, part, rows // part, tokens), bf16),
            pltpu.VMEM((outer, part, rows // part, inner * tokens), bf16),
            pltpu.VMEM((inner, message, 2 * HEAD), bf16),
            pltpu.VMEM((inner, message, 2 * HEAD), bf16),
            pltpu.VMEM((message, 2 * HEAD), bf16),
            pltpu.VMEM((message, 2 * HEAD), bf16),
            pltpu.VMEM((outer, message, 2 * HEAD), bf16),
            pltpu.VMEM((outer, message, 2 * HEAD), bf16),
            pltpu.VMEM((inner, 2, width, tokens), bf16),
            pltpu.VMEM((width, inner * tokens), bf16),
            pltpu.VMEM((n_tp - 1, width, tokens), bf16),
            pltpu.VMEM((outer, width, rows), bf16),
            pltpu.VMEM((outer - 1, width, rows), bf16),
            pltpu.VMEM((n_tp, tokens, width), bf16),
            dma((n_tp - 1,)), dma((n_tp - 1,)),
            dma((inner - 1,)), dma((inner - 1,)),
            dma((1,)), dma((1,)),
            dma((inner - 1,)), dma((inner - 1,)),
            dma((inner - 1,)), dma((inner - 1,)),
            dma((outer - 1,)), dma((outer - 1,)),
            dma((outer - 1,)), dma((outer - 1,)),
            dma((inner - 1,)), dma((inner - 1,)),
            dma((n_tp - 1,)), dma((n_tp - 1,)),
            dma((outer - 1,)), dma((outer - 1,)),
        ],
        compiler_params=pltpu.CompilerParams(
            collective_id=0, has_side_effects=True, vmem_limit_bytes=60 * 1024 * 1024
        ),
    )(block_input, value_weight.T, query_pre.T, forget_pre.T, lower_bound[None, :], out_grad.T)
    return gq.T, gf.T, gx, gw.T


def solution(mesh):
    n, n_tp = mesh.shape["sp"], mesh.shape["tp"]
    in_specs = (P("sp", None), P(None, "tp"), P("sp", "tp"), P("sp", "tp"), P("tp"), P("sp", "tp"))
    out_specs = (P("sp", "tp"), P("sp", "tp"), P(("sp", "tp"), None), P("sp", "tp"))
    return jax.shard_map(
        functools.partial(on_device, n, n_tp),
        mesh=mesh, in_specs=in_specs, out_specs=out_specs, check_vma=False,
    )
```

```python
import functools

import jax
import jax.numpy as jnp
from jax import lax
from jax.experimental import pallas as pl
from jax.experimental.pallas import tpu as pltpu
from jax.sharding import PartitionSpec as P

HEAD = 64
MESH = pl.DeviceIdType.MESH
f32, bf16 = jnp.float32, jnp.bfloat16
LOGROWS = 16


def nn(a, b):
    return lax.dot_general(a, b, (((1,), (0,)), ((), ())), preferred_element_type=f32)


def nt(a, b):
    return lax.dot_general(a, b, (((1,), (1,)), ((), ())), preferred_element_type=f32)


def tn(a, b):
    return lax.dot_general(a, b, (((0,), (0,)), ((), ())), preferred_element_type=f32)


def split(a):
    high = a.astype(bf16)
    return high, (a - high.astype(f32)).astype(bf16)


def kernel(
    inner, outer, n_tp, part,
    x_in, w_in, q_hbm, f_hbm, lb_ref, g_in,
    gq_ref, gf_ref, gx_ref, gw_ref,
    x_ref, w_ref, q_ref, f_ref, g_ref, in_sem,
    w_all, xt, xg, b1, f1, bmsg, fmsg, b2, f2, gvk, dvp, dvm, pmsg, pin, dvs,
    w_send, w_recv, x_send, x_recv, r_send, r_recv, b1_send, b1_recv, f1_send, f1_recv,
    b2_send, b2_recv, f2_send, f2_recv, k_send, k_recv, m_send, m_recv, p_send, p_recv,
):
    me, core = lax.axis_index("sp"), lax.axis_index("tp")
    here, plane = lax.rem(me, inner), me // inner
    tokens, depth = x_ref.shape
    width = q_ref.shape[0]
    heads = width // HEAD
    half = tokens // n_tp
    pairs, odd = heads // 2, heads % 2
    wide = 2 * HEAD
    packed = pairs * HEAD + odd * HEAD // 2

    def near(k):
        return (plane * inner + lax.rem(here + k, inner), core)

    def column(k):
        return (lax.rem(plane + k, outer) * inner + here, core)

    def mate(k):
        return (me, lax.rem(core + k, n_tp))

    def rc(src, dst, send, recv, k, to):
        return pltpu.make_async_remote_copy(src, dst, send.at[k - 1], recv.at[k - 1], to, MESH)

    loads = [
        pltpu.make_async_copy(src, dst, in_sem.at[i])
        for i, (src, dst) in enumerate(
            ((f_hbm, f_ref), (q_hbm, q_ref), (g_in, g_ref), (w_in, w_ref), (x_in, x_ref))
        )
    ]
    for load in loads:
        load.start()
    barrier = pltpu.get_barrier_semaphore()
    for to, count in ((near, inner), (column, outer), (mate, n_tp)):
        for k in range(1, count):
            pl.semaphore_signal(barrier, inc=1, device_id=to(k), device_id_type=MESH)

    lead = core * (part - 1)
    own_lanes = pl.ds(pl.multiple_of(here * tokens, tokens), tokens)

    def copy_w(k):
        return rc(w_ref, w_all.at[k - 1], w_send, w_recv, k, mate(k))

    def copy_x(k):
        return rc(
            xt.at[:, lax.rem(here + k, inner), lead], xg.at[:, lead, :, own_lanes],
            x_send, x_recv, k, near(k),
        )

    def copy_r(lane):
        return rc(xg.at[:, lane], xg.at[:, lane], r_send, r_recv, 1, mate(1))

    def copy_b1(k, at):
        return rc(b1.at[at], b1.at[at], b1_send, b1_recv, k, near(k))

    def copy_f1(k, at):
        return rc(f1.at[at], f1.at[at], f1_send, f1_recv, k, near(k))

    def copy_k(k, at, h):
        each_h = (inner - 1) * h + k
        return rc(gvk.at[at, h], gvk.at[at, h], k_send, k_recv, each_h, near(k))

    def copy_b2(k, at):
        return rc(bmsg, b2.at[at], b2_send, b2_recv, k, column(k))

    def copy_f2(k, at):
        return rc(fmsg, f2.at[at], f2_send, f2_recv, k, column(k))

    def copy_m(k):
        return rc(dvp.at[:, own_lanes], dvm.at[k - 1], m_send, m_recv, k, mate(k))

    def copy_p(k, h):
        return rc(
            pmsg.at[h, lax.rem(plane + k, outer)], pin.at[k - 1, h],
            p_send, p_recv, (outer - 1) * h + k, column(k),
        )

    def source(k):
        return lax.rem(here + inner - k, inner)

    lane_low = lax.broadcasted_iota(jnp.int32, (1, wide), 1) < HEAD

    def pairs_of(a, j):
        return a[j * wide : (j + 1) * wide, :]

    def twice(a):
        return jnp.concatenate([a[pairs * wide :, :]] * 2, axis=0)

    def pack(values, keys):
        out = []
        for j in range(pairs):
            full = nt(pairs_of(values, j), pairs_of(keys, j))
            out.append(jnp.where(lane_low, full[:HEAD, :], full[HEAD:, :]))
        if odd:
            full = nt(values[pairs * wide :, :], twice(keys))
            out.append(jnp.where(lane_low, full[: HEAD // 2, :], full[HEAD // 2 :, :]))
        return jnp.concatenate(out, axis=0)

    def opened(state):
        out = []
        for j in range(pairs + odd):
            size = HEAD if j < pairs else HEAD // 2
            rows_of = state[j * HEAD : j * HEAD + size, :]
            out.append(
                jnp.concatenate(
                    [jnp.where(lane_low, rows_of, 0.0), jnp.where(lane_low, 0.0, rows_of)], axis=0
                ).astype(bf16)
            )
        return out

    def from_values(blocks, a):
        out = [tn(blocks[j], pairs_of(a, j)) for j in range(pairs)]
        if odd:
            full = tn(blocks[pairs], a[pairs * wide :, :])
            out.append(full[:HEAD, :] + full[HEAD:, :])
        return jnp.concatenate(out, axis=0)

    def scaled(logs, state):
        out = []
        for j in range(pairs + odd):
            size = HEAD if j < pairs else HEAD // 2
            out.append(jnp.exp(logs[j]) * state[j * HEAD : j * HEAD + size, :])
        return jnp.concatenate(out, axis=0)

    row_at = lax.broadcasted_iota(jnp.int32, (LOGROWS, wide), 0)

    def log_rows(logs):
        rows_f = jnp.zeros((LOGROWS, wide), f32)
        for j, log in enumerate(logs):
            high, low = split(log)
            rows_f = jnp.where(row_at == 2 * j, high.astype(f32), rows_f)
            rows_f = jnp.where(row_at == 2 * j + 1, low.astype(f32), rows_f)
        return rows_f.astype(bf16)

    def read(ref, at):
        state = ref[at, 0:packed, :].astype(f32)
        tail = ref[at, packed : packed + LOGROWS, :].astype(f32)
        logs = [tail[2 * j : 2 * j + 1, :] + tail[2 * j + 1 : 2 * j + 2, :] for j in range(pairs + odd)]
        return state, logs

    def added(a, b):
        return [p + q for p, q in zip(a, b)]

    s_at = lax.broadcasted_iota(jnp.int32, (tokens, tokens), 0)
    t_at = lax.broadcasted_iota(jnp.int32, (tokens, tokens), 1)
    upper, lower = s_at <= t_at, s_at >= t_at
    upper_b, lower_b = upper.astype(f32).astype(bf16), lower.astype(f32).astype(bf16)
    ones = jnp.ones((LOGROWS, tokens), bf16)
    lb = jnp.broadcast_to(lb_ref[...], (tokens, width)).T
    loads[0].wait()
    f_in = f_ref[...].astype(f32)
    f_sig = jax.nn.sigmoid(f_in)
    key = (1.0 - lb) * jax.nn.sigmoid(-f_in)
    high, low = split(jnp.log1p(-key))
    cumulative = nn(high, upper_b) + nn(low, upper_b)
    growth = jnp.exp(cumulative)
    loads[1].wait()
    q_in = q_ref[...].astype(f32)
    q_sig = jax.nn.sigmoid(q_in)
    query = q_in * q_sig
    q_dec = (query * growth).astype(bf16)
    loads[2].wait()
    g = g_ref[...]
    logs = []
    for j in range(pairs):
        logs.append((nt(ones, pairs_of(high, j)) + nt(ones, pairs_of(low, j)))[0:1, :])
    if odd:
        logs.append((nt(ones, twice(high)) + nt(ones, twice(low)))[0:1, :])
    tail = log_rows(logs)
    b1[here, 0:packed, :] = pack(g, q_dec).astype(bf16)
    b1[here, packed : packed + LOGROWS, :] = tail
    pl.semaphore_wait(barrier, inner + outer + n_tp - 3)
    for k in range(1, inner):
        copy_b1(k, here).start()
    loads[3].wait()
    for k in range(1, n_tp):
        copy_w(k).start()
    loads[4].wait()

    value = nt(w_ref[...], x_ref[...]).astype(bf16)
    closing = cumulative[:, tokens - 1 : tokens]
    k_end = (key * jnp.exp(closing - cumulative)).astype(bf16)
    update = pack(value, k_end)
    f1[here, 0:packed, :] = update.astype(bf16)
    f1[here, packed : packed + LOGROWS, :] = tail
    for k in range(1, inner):
        copy_f1(k, here).start()
    shrinking = jnp.exp(-cumulative)
    k_dec = (key * shrinking).astype(bf16)

    def of(a, h):
        return a[h * HEAD : (h + 1) * HEAD, :]

    xt[...] = x_ref[...].T.reshape(xt.shape)
    for k in range(1, inner):
        copy_x(k).start()
    xg[:, lead, :, own_lanes] = xt[:, here, lead]
    for h in range(heads):
        mixing = jnp.where(upper, tn(of(k_dec, h), of(q_dec, h)), 0.0).astype(bf16)
        gvk[here, h, 0] = nt(of(g, h), mixing).astype(bf16)
        gvk[here, h, 1] = of(k_end, h)
        for k in range(1, inner):
            copy_k(k, here, h).start()

    for k in range(1, inner):
        copy_b1(k, source(k)).wait_recv()
    inside, after = [None] * inner, [None] * inner
    running = jnp.zeros((packed, wide), f32)
    plane_logs = [jnp.zeros((1, wide), f32) for _ in range(pairs + odd)]
    for j in reversed(range(inner)):
        inside[j], after[j] = running, plane_logs
        state, own_logs = read(b1, j)
        running = state + scaled(own_logs, running)
        plane_logs = added(plane_logs, own_logs)
    plane_tail = log_rows(plane_logs)
    bmsg[0:packed, :] = running.astype(bf16)
    bmsg[packed : packed + LOGROWS, :] = plane_tail

    def each(lo, hi, act):
        def step(i, carried):
            act(i)
            return carried

        lax.fori_loop(lo, hi, step, 0)

    each(outer - plane, outer, lambda k: copy_b2(k, plane).start())

    for k in range(1, inner):
        copy_f1(k, source(k)).wait_recv()
    running = jnp.zeros((packed, wide), f32)
    before = [jnp.zeros((1, wide), f32) for _ in range(pairs + odd)]
    incoming = running
    in_logs = before
    for j in range(inner):
        incoming = jnp.where(here == j, running, incoming)
        in_logs = [jnp.where(here == j, p, q) for p, q in zip(before, in_logs)]
        state, own_logs = read(f1, j)
        running = state + scaled(own_logs, running)
        before = added(before, own_logs)
    fmsg[0:packed, :] = running.astype(bf16)
    fmsg[packed : packed + LOGROWS, :] = plane_tail
    each(1, outer - plane, lambda k: copy_f2(k, plane).start())

    pairing = [jnp.where(upper, tn(of(value, h), of(g, h)), 0.0).astype(bf16) for h in range(heads)]
    gk_local = jnp.concatenate([nt(of(q_dec, h), pairing[h]) for h in range(heads)], axis=0)
    gq_local = jnp.concatenate([nn(of(k_dec, h), pairing[h]) for h in range(heads)], axis=0)

    for k in range(1, inner):
        lanes = pl.ds(pl.multiple_of(source(k) * tokens, tokens), tokens)
        rc(xt.at[:, 0, lead], xg.at[:, lead, :, lanes], x_send, x_recv, k, near(k)).wait_recv()
    if part > 1:
        copy_r(lead).start()

    empty = jnp.zeros((packed, wide), f32)
    none = [jnp.zeros((1, wide), f32) for _ in range(pairs + odd)]

    def entering(ref, copy, count, place, distance):
        def step(i, carried):
            total, weight = carried
            copy(distance(i), place(i)).wait_recv()
            state, own_logs = read(ref, place(i))
            return total + scaled(weight, state), added(weight, own_logs)

        return lax.fori_loop(0, count, step, (empty, none))[0]

    below = entering(
        b2, copy_b2, outer - 1 - plane, lambda i: plane + 1 + i, lambda i: outer - 1 - i
    )
    outgoing = empty
    opens = []
    for j in range(inner):
        grad_state = inside[j] + scaled(after[j], below)
        outgoing = jnp.where(here == j, grad_state, outgoing)
        opens.append(opened(grad_state))
    if part > 1:
        copy_r(1 - lead).wait_recv()
    for h in range(heads):
        for k in range(1, inner):
            copy_k(k, source(k), h).wait_recv()
        at = slice(h * HEAD, (h + 1) * HEAD)
        for j in range(inner):
            block = opens[j][h // 2][h % 2 * HEAD : (h % 2 + 1) * HEAD, :]
            doubled = jnp.concatenate([gvk[j, h, 1]] * 2, axis=0)
            value_grad = gvk[j, h, 0].astype(f32) + nn(block, doubled)
            dvp[at, j * tokens : (j + 1) * tokens] = value_grad.astype(bf16)
        for z in range(outer):
            pieces = [nt(dvp[at, :], xg[z, p]) for p in range(part)]
            pmsg[h, z] = jnp.concatenate(pieces, axis=1).astype(bf16)
        for k in reversed(range(1, outer)):
            copy_p(k, h).start()
    for k in range(1, n_tp):
        copy_m(k).start()

    def rows_half(a, slot):
        dvs[slot] = a.T
        return dvs[slot, pl.ds(pl.multiple_of(core * half, half), half), :]

    gx = nn(rows_half(dvp[:, own_lanes], 0), w_ref[...]).astype(bf16).astype(f32)
    for k in range(1, n_tp):
        copy_w(k).wait_recv()
        copy_m(k).wait_recv()
        gx = gx + nn(rows_half(dvm[k - 1], k), w_all[k - 1]).astype(bf16).astype(f32)
    gx_ref[...] = gx.astype(bf16)

    above = entering(f2, copy_f2, plane, lambda i: plane - 1 - i, lambda i: i + 1)
    incoming = incoming + scaled(in_logs, above)
    grad_query = growth * (gq_local + from_values(opened(incoming), g))
    remaining = jnp.exp(closing - cumulative)
    grad_key = shrinking * gk_local + remaining * from_values(opened(outgoing), value)
    product = outgoing * (scaled(logs, incoming) + update)
    p_high, p_low = split(product)
    bound = []
    for j in range(pairs + odd):
        size = HEAD if j < pairs else HEAD // 2
        every = jnp.ones((size, tokens), bf16)
        at = slice(j * HEAD, j * HEAD + size)
        full = tn(p_high[at, :], every) + tn(p_low[at, :], every)
        bound.append(full if j < pairs else full[:HEAD, :] + full[HEAD:, :])
    boundary = jnp.concatenate(bound, axis=0)
    c_high, c_low = split(query * grad_query - key * grad_key)
    grad_decay = nn(c_high, lower_b) + nn(c_low, lower_b) + boundary
    gq_ref[...] = (grad_query * (q_sig * (1.0 + q_in * (1.0 - q_sig)))).astype(bf16)
    gf_ref[...] = (-(grad_key - grad_decay / (1.0 - key)) * key * f_sig).astype(bf16)

    for h in range(heads):
        total = pmsg[h, plane].astype(f32)
        for k in range(1, outer):
            copy_p(k, h).wait_recv()
            total = total + pin[k - 1, h].astype(f32)
        gw_ref[h * HEAD : (h + 1) * HEAD, :] = total

    for k in range(1, n_tp):
        copy_w(k).wait_send()
        copy_m(k).wait_send()
    if part > 1:
        copy_r(lead).wait_send()
    for k in range(1, inner):
        copy_b1(k, here).wait_send()
        copy_f1(k, here).wait_send()
        for h in range(heads):
            copy_k(k, here, h).wait_send()
        copy_x(k).wait_send()
    each(outer - plane, outer, lambda k: copy_b2(k, plane).wait_send())
    each(1, outer - plane, lambda k: copy_f2(k, plane).wait_send())
    for k in range(1, outer):
        for h in range(heads):
            copy_p(k, h).wait_send()


def hand_on(*refs):
    for source, target in zip(refs[:4], refs[4:]):
        target[...] = source[...]


def on_device(n, n_tp, block_input, value_weight, query_pre, forget_pre, lower_bound, out_grad):
    tokens, depth = block_input.shape
    width = query_pre.shape[1]
    heads = width // HEAD
    rows = depth // n
    inner = 1
    while n % (inner * 2) == 0 and (inner * 2) ** 2 <= n:
        inner *= 2
    outer = n // inner
    part = 2 if n_tp == 2 and rows % 32 == 0 else 1
    message = (heads // 2) * HEAD + (heads % 2) * HEAD // 2 + LOGROWS
    dma = pltpu.SemaphoreType.DMA
    vmem = pl.BlockSpec(memory_space=pltpu.VMEM)
    anywhere = pl.BlockSpec(memory_space=pl.ANY)
    results = pl.pallas_call(
        functools.partial(kernel, inner, outer, n_tp, part),
        out_shape=(
            jax.ShapeDtypeStruct((width, tokens), bf16),
            jax.ShapeDtypeStruct((width, tokens), bf16),
            jax.ShapeDtypeStruct((tokens // n_tp, depth), bf16),
            jax.ShapeDtypeStruct((width, rows), f32),
        ),
        in_specs=[anywhere] * 4 + [vmem, anywhere],
        out_specs=(vmem,) * 4,
        scratch_shapes=[
            pltpu.VMEM((tokens, depth), bf16),
            pltpu.VMEM((width, depth), bf16),
            pltpu.VMEM((width, tokens), bf16),
            pltpu.VMEM((width, tokens), bf16),
            pltpu.VMEM((width, tokens), bf16),
            dma((5,)),
            pltpu.VMEM((n_tp - 1, width, depth), bf16),
            pltpu.VMEM((outer, inner, part, rows // part, tokens), bf16),
            pltpu.VMEM((outer, part, rows // part, inner * tokens), bf16),
            pltpu.VMEM((inner, message, 2 * HEAD), bf16),
            pltpu.VMEM((inner, message, 2 * HEAD), bf16),
            pltpu.VMEM((message, 2 * HEAD), bf16),
            pltpu.VMEM((message, 2 * HEAD), bf16),
            pltpu.VMEM((outer, message, 2 * HEAD), bf16),
            pltpu.VMEM((outer, message, 2 * HEAD), bf16),
            pltpu.VMEM((inner, heads, 2, HEAD, tokens), bf16),
            pltpu.VMEM((width, inner * tokens), bf16),
            pltpu.VMEM((n_tp - 1, width, tokens), bf16),
            pltpu.VMEM((heads, outer, HEAD, rows), bf16),
            pltpu.VMEM((outer - 1, heads, HEAD, rows), bf16),
            pltpu.VMEM((n_tp, tokens, width), bf16),
            dma((n_tp - 1,)), dma((n_tp - 1,)),
            dma((inner - 1,)), dma((inner - 1,)),
            dma((1,)), dma((1,)),
            dma((inner - 1,)), dma((inner - 1,)),
            dma((inner - 1,)), dma((inner - 1,)),
            dma((outer - 1,)), dma((outer - 1,)),
            dma((outer - 1,)), dma((outer - 1,)),
            dma((heads * (inner - 1),)), dma((heads * (inner - 1),)),
            dma((n_tp - 1,)), dma((n_tp - 1,)),
            dma((heads * (outer - 1),)), dma((heads * (outer - 1),)),
        ],
        compiler_params=pltpu.CompilerParams(
            collective_id=0, has_side_effects=True, vmem_limit_bytes=60 * 1024 * 1024
        ),
    )(block_input, value_weight.T, query_pre.T, forget_pre.T, lower_bound[None, :], out_grad.T)
    gq, gf, gx, gw = pl.pallas_call(
        hand_on,
        out_shape=tuple(jax.ShapeDtypeStruct(a.shape, a.dtype) for a in results),
        in_specs=[vmem] * 4,
        out_specs=(vmem,) * 4,
    )(*results)
    return gq.T, gf.T, gx, gw.T


def solution(mesh):
    n, n_tp = mesh.shape["sp"], mesh.shape["tp"]
    in_specs = (P("sp", None), P(None, "tp"), P("sp", "tp"), P("sp", "tp"), P("tp"), P("sp", "tp"))
    out_specs = (P("sp", "tp"), P("sp", "tp"), P(("sp", "tp"), None), P("sp", "tp"))
    return jax.shard_map(
        functools.partial(on_device, n, n_tp),
        mesh=mesh, in_specs=in_specs, out_specs=out_specs, check_vma=False,
    )
```

```python
import functools

import jax
import jax.numpy as jnp
from jax import lax
from jax.experimental import pallas as pl
from jax.experimental.pallas import tpu as pltpu
from jax.sharding import PartitionSpec as P

HEAD = 64
MESH = pl.DeviceIdType.MESH
f32, bf16 = jnp.float32, jnp.bfloat16
LOGROWS = 16


def nn(a, b):
    return lax.dot_general(a, b, (((1,), (0,)), ((), ())), preferred_element_type=f32)


def nt(a, b):
    return lax.dot_general(a, b, (((1,), (1,)), ((), ())), preferred_element_type=f32)


def tn(a, b):
    return lax.dot_general(a, b, (((0,), (0,)), ((), ())), preferred_element_type=f32)


def split(a):
    high = a.astype(bf16)
    return high, (a - high.astype(f32)).astype(bf16)


def kernel(
    inner, outer, n_tp, part,
    x_in, w_in, q_hbm, f_hbm, lb_ref, g_in,
    gq_ref, gf_ref, gx_ref, gw_ref,
    x_ref, w_ref, q_ref, f_ref, g_ref, in_sem,
    w_all, xt, xg, b1, f1, bmsg, fmsg, b2, f2, gvk, dvp, dvm, pmsg, pin, dvs,
    w_send, w_recv, x_send, x_recv, r_send, r_recv, b1_send, b1_recv, f1_send, f1_recv,
    b2_send, b2_recv, f2_send, f2_recv, k_send, k_recv, m_send, m_recv, p_send, p_recv,
):
    me, core = lax.axis_index("sp"), lax.axis_index("tp")
    here, plane = lax.rem(me, inner), me // inner
    tokens, depth = x_ref.shape
    width = q_ref.shape[0]
    heads = width // HEAD
    half = tokens // n_tp
    pairs, odd = heads // 2, heads % 2
    wide = 2 * HEAD
    packed = pairs * HEAD + odd * HEAD // 2

    def near(k):
        return (plane * inner + lax.rem(here + k, inner), core)

    def column(k):
        return (lax.rem(plane + k, outer) * inner + here, core)

    def mate(k):
        return (me, lax.rem(core + k, n_tp))

    def rc(src, dst, send, recv, k, to):
        return pltpu.make_async_remote_copy(src, dst, send.at[k - 1], recv.at[k - 1], to, MESH)

    loads = [
        pltpu.make_async_copy(src, dst, in_sem.at[i])
        for i, (src, dst) in enumerate(
            ((f_hbm, f_ref), (q_hbm, q_ref), (g_in, g_ref), (w_in, w_ref), (x_in, x_ref))
        )
    ]
    for load in loads:
        load.start()
    barrier = pltpu.get_barrier_semaphore()
    for to, count in ((near, inner), (column, outer), (mate, n_tp)):
        for k in range(1, count):
            pl.semaphore_signal(barrier, inc=1, device_id=to(k), device_id_type=MESH)

    lead = core * (part - 1)
    own_lanes = pl.ds(pl.multiple_of(here * tokens, tokens), tokens)

    def copy_w(k):
        return rc(w_ref, w_all.at[k - 1], w_send, w_recv, k, mate(k))

    def copy_x(k):
        return rc(
            xt.at[:, lax.rem(here + k, inner), lead], xg.at[:, lead, :, own_lanes],
            x_send, x_recv, k, near(k),
        )

    def copy_r(lane):
        return rc(xg.at[:, lane], xg.at[:, lane], r_send, r_recv, 1, mate(1))

    def copy_b1(k, at):
        return rc(b1.at[at], b1.at[at], b1_send, b1_recv, k, near(k))

    def copy_f1(k, at):
        return rc(f1.at[at], f1.at[at], f1_send, f1_recv, k, near(k))

    def copy_k(k, at, h):
        each_h = (inner - 1) * h + k
        return rc(gvk.at[at, h], gvk.at[at, h], k_send, k_recv, each_h, near(k))

    def copy_b2(k, at):
        return rc(bmsg, b2.at[at], b2_send, b2_recv, k, column(k))

    def copy_f2(k, at):
        return rc(fmsg, f2.at[at], f2_send, f2_recv, k, column(k))

    def copy_m(k):
        return rc(dvp.at[:, own_lanes], dvm.at[k - 1], m_send, m_recv, k, mate(k))

    def copy_p(k, h):
        return rc(
            pmsg.at[h, lax.rem(plane + k, outer)], pin.at[k - 1, h],
            p_send, p_recv, (outer - 1) * h + k, column(k),
        )

    def source(k):
        return lax.rem(here + inner - k, inner)

    lane_low = lax.broadcasted_iota(jnp.int32, (1, wide), 1) < HEAD

    def pairs_of(a, j):
        return a[j * wide : (j + 1) * wide, :]

    def twice(a):
        return jnp.concatenate([a[pairs * wide :, :]] * 2, axis=0)

    def pack(values, keys):
        out = []
        for j in range(pairs):
            full = nt(pairs_of(values, j), pairs_of(keys, j))
            out.append(jnp.where(lane_low, full[:HEAD, :], full[HEAD:, :]))
        if odd:
            full = nt(values[pairs * wide :, :], twice(keys))
            out.append(jnp.where(lane_low, full[: HEAD // 2, :], full[HEAD // 2 :, :]))
        return jnp.concatenate(out, axis=0)

    def opened(state):
        out = []
        for j in range(pairs + odd):
            size = HEAD if j < pairs else HEAD // 2
            rows_of = state[j * HEAD : j * HEAD + size, :]
            out.append(
                jnp.concatenate(
                    [jnp.where(lane_low, rows_of, 0.0), jnp.where(lane_low, 0.0, rows_of)], axis=0
                ).astype(bf16)
            )
        return out

    def from_values(blocks, a):
        out = [tn(blocks[j], pairs_of(a, j)) for j in range(pairs)]
        if odd:
            full = tn(blocks[pairs], a[pairs * wide :, :])
            out.append(full[:HEAD, :] + full[HEAD:, :])
        return jnp.concatenate(out, axis=0)

    def scaled(logs, state):
        out = []
        for j in range(pairs + odd):
            size = HEAD if j < pairs else HEAD // 2
            out.append(jnp.exp(logs[j]) * state[j * HEAD : j * HEAD + size, :])
        return jnp.concatenate(out, axis=0)

    row_at = lax.broadcasted_iota(jnp.int32, (LOGROWS, wide), 0)

    def log_rows(logs):
        rows_f = jnp.zeros((LOGROWS, wide), f32)
        for j, log in enumerate(logs):
            high, low = split(log)
            rows_f = jnp.where(row_at == 2 * j, high.astype(f32), rows_f)
            rows_f = jnp.where(row_at == 2 * j + 1, low.astype(f32), rows_f)
        return rows_f.astype(bf16)

    def read(ref, at):
        state = ref[at, 0:packed, :].astype(f32)
        tail = ref[at, packed : packed + LOGROWS, :].astype(f32)
        logs = [tail[2 * j : 2 * j + 1, :] + tail[2 * j + 1 : 2 * j + 2, :] for j in range(pairs + odd)]
        return state, logs

    def added(a, b):
        return [p + q for p, q in zip(a, b)]

    s_at = lax.broadcasted_iota(jnp.int32, (tokens, tokens), 0)
    t_at = lax.broadcasted_iota(jnp.int32, (tokens, tokens), 1)
    upper, lower = s_at <= t_at, s_at >= t_at
    upper_b, lower_b = upper.astype(f32).astype(bf16), lower.astype(f32).astype(bf16)
    ones = jnp.ones((LOGROWS, tokens), bf16)
    lb = jnp.broadcast_to(lb_ref[...], (tokens, width)).T
    loads[0].wait()
    f_in = f_ref[...].astype(f32)
    f_sig = jax.nn.sigmoid(f_in)
    key = (1.0 - lb) * jax.nn.sigmoid(-f_in)
    high, low = split(jnp.log1p(-key))
    cumulative = nn(high, upper_b) + nn(low, upper_b)
    growth = jnp.exp(cumulative)
    loads[1].wait()
    q_in = q_ref[...].astype(f32)
    q_sig = jax.nn.sigmoid(q_in)
    query = q_in * q_sig
    q_dec = (query * growth).astype(bf16)
    loads[2].wait()
    g = g_ref[...]
    logs = []
    for j in range(pairs):
        logs.append((nt(ones, pairs_of(high, j)) + nt(ones, pairs_of(low, j)))[0:1, :])
    if odd:
        logs.append((nt(ones, twice(high)) + nt(ones, twice(low)))[0:1, :])
    tail = log_rows(logs)
    b1[here, 0:packed, :] = pack(g, q_dec).astype(bf16)
    b1[here, packed : packed + LOGROWS, :] = tail
    pl.semaphore_wait(barrier, inner + outer + n_tp - 3)
    for k in range(1, inner):
        copy_b1(k, here).start()
    loads[3].wait()
    for k in range(1, n_tp):
        copy_w(k).start()
    loads[4].wait()

    value = nt(w_ref[...], x_ref[...]).astype(bf16)
    closing = cumulative[:, tokens - 1 : tokens]
    k_end = (key * jnp.exp(closing - cumulative)).astype(bf16)
    update = pack(value, k_end)
    f1[here, 0:packed, :] = update.astype(bf16)
    f1[here, packed : packed + LOGROWS, :] = tail
    for k in range(1, inner):
        copy_f1(k, here).start()
    shrinking = jnp.exp(-cumulative)
    k_dec = (key * shrinking).astype(bf16)

    def of(a, h):
        return a[h * HEAD : (h + 1) * HEAD, :]

    xt[...] = x_ref[...].T.reshape(xt.shape)
    for k in range(1, inner):
        copy_x(k).start()
    xg[:, lead, :, own_lanes] = xt[:, here, lead]
    for h in range(heads):
        mixing = jnp.where(upper, tn(of(k_dec, h), of(q_dec, h)), 0.0).astype(bf16)
        gvk[here, h, 0] = nt(of(g, h), mixing).astype(bf16)
        gvk[here, h, 1] = of(k_end, h)
        for k in range(1, inner):
            copy_k(k, here, h).start()

    for k in range(1, inner):
        copy_b1(k, source(k)).wait_recv()
    inside, after = [None] * inner, [None] * inner
    running = jnp.zeros((packed, wide), f32)
    plane_logs = [jnp.zeros((1, wide), f32) for _ in range(pairs + odd)]
    for j in reversed(range(inner)):
        inside[j], after[j] = running, plane_logs
        state, own_logs = read(b1, j)
        running = state + scaled(own_logs, running)
        plane_logs = added(plane_logs, own_logs)
    plane_tail = log_rows(plane_logs)
    bmsg[0:packed, :] = running.astype(bf16)
    bmsg[packed : packed + LOGROWS, :] = plane_tail

    def each(lo, hi, act):
        def step(i, carried):
            act(i)
            return carried

        lax.fori_loop(lo, hi, step, 0)

    each(outer - plane, outer, lambda k: copy_b2(k, plane).start())

    for k in range(1, inner):
        copy_f1(k, source(k)).wait_recv()
    running = jnp.zeros((packed, wide), f32)
    before = [jnp.zeros((1, wide), f32) for _ in range(pairs + odd)]
    incoming = running
    in_logs = before
    for j in range(inner):
        incoming = jnp.where(here == j, running, incoming)
        in_logs = [jnp.where(here == j, p, q) for p, q in zip(before, in_logs)]
        state, own_logs = read(f1, j)
        running = state + scaled(own_logs, running)
        before = added(before, own_logs)
    fmsg[0:packed, :] = running.astype(bf16)
    fmsg[packed : packed + LOGROWS, :] = plane_tail
    each(1, outer - plane, lambda k: copy_f2(k, plane).start())

    pairing = [jnp.where(upper, tn(of(value, h), of(g, h)), 0.0).astype(bf16) for h in range(heads)]
    gk_local = jnp.concatenate([nt(of(q_dec, h), pairing[h]) for h in range(heads)], axis=0)
    gq_local = jnp.concatenate([nn(of(k_dec, h), pairing[h]) for h in range(heads)], axis=0)

    for k in range(1, inner):
        lanes = pl.ds(pl.multiple_of(source(k) * tokens, tokens), tokens)
        rc(xt.at[:, 0, lead], xg.at[:, lead, :, lanes], x_send, x_recv, k, near(k)).wait_recv()
    if part > 1:
        copy_r(lead).start()

    empty = jnp.zeros((packed, wide), f32)
    none = [jnp.zeros((1, wide), f32) for _ in range(pairs + odd)]

    def entering(ref, copy, count, place, distance):
        def step(i, carried):
            total, weight = carried
            copy(distance(i), place(i)).wait_recv()
            state, own_logs = read(ref, place(i))
            return total + scaled(weight, state), added(weight, own_logs)

        return lax.fori_loop(0, count, step, (empty, none))[0]

    below = entering(
        b2, copy_b2, outer - 1 - plane, lambda i: plane + 1 + i, lambda i: outer - 1 - i
    )
    outgoing = empty
    opens = []
    for j in range(inner):
        grad_state = inside[j] + scaled(after[j], below)
        outgoing = jnp.where(here == j, grad_state, outgoing)
        opens.append(opened(grad_state))
    if part > 1:
        copy_r(1 - lead).wait_recv()
    for h in range(heads):
        for k in range(1, inner):
            copy_k(k, source(k), h).wait_recv()
        at = slice(h * HEAD, (h + 1) * HEAD)
        for j in range(inner):
            block = opens[j][h // 2][h % 2 * HEAD : (h % 2 + 1) * HEAD, :]
            doubled = jnp.concatenate([gvk[j, h, 1]] * 2, axis=0)
            value_grad = gvk[j, h, 0].astype(f32) + nn(block, doubled)
            dvp[at, j * tokens : (j + 1) * tokens] = value_grad.astype(bf16)
        for z in range(outer):
            pieces = [nt(dvp[at, :], xg[z, p]) for p in range(part)]
            pmsg[h, z] = jnp.concatenate(pieces, axis=1).astype(bf16)
        for k in reversed(range(1, outer)):
            copy_p(k, h).start()
    for k in range(1, n_tp):
        copy_m(k).start()

    def rows_half(a, slot):
        dvs[slot] = a.T
        return dvs[slot, pl.ds(pl.multiple_of(core * half, half), half), :]

    gx = nn(rows_half(dvp[:, own_lanes], 0), w_ref[...]).astype(bf16).astype(f32)
    for k in range(1, n_tp):
        copy_w(k).wait_recv()
        copy_m(k).wait_recv()
        gx = gx + nn(rows_half(dvm[k - 1], k), w_all[k - 1]).astype(bf16).astype(f32)
    gx_ref[...] = gx.astype(bf16)

    above = entering(f2, copy_f2, plane, lambda i: plane - 1 - i, lambda i: i + 1)
    incoming = incoming + scaled(in_logs, above)
    grad_query = growth * (gq_local + from_values(opened(incoming), g))
    remaining = jnp.exp(closing - cumulative)
    grad_key = shrinking * gk_local + remaining * from_values(opened(outgoing), value)
    product = outgoing * (scaled(logs, incoming) + update)
    p_high, p_low = split(product)
    bound = []
    for j in range(pairs + odd):
        size = HEAD if j < pairs else HEAD // 2
        every = jnp.ones((size, tokens), bf16)
        at = slice(j * HEAD, j * HEAD + size)
        full = tn(p_high[at, :], every) + tn(p_low[at, :], every)
        bound.append(full if j < pairs else full[:HEAD, :] + full[HEAD:, :])
    boundary = jnp.concatenate(bound, axis=0)
    c_high, c_low = split(query * grad_query - key * grad_key)
    grad_decay = nn(c_high, lower_b) + nn(c_low, lower_b) + boundary
    gq_ref[...] = (grad_query * (q_sig * (1.0 + q_in * (1.0 - q_sig)))).astype(bf16)
    gf_ref[...] = (-(grad_key - grad_decay / (1.0 - key)) * key * f_sig).astype(bf16)

    for h in range(heads):
        total = pmsg[h, plane].astype(f32)
        for k in range(1, outer):
            copy_p(k, h).wait_recv()
            total = total + pin[k - 1, h].astype(f32)
        gw_ref[h * HEAD : (h + 1) * HEAD, :] = total

    for k in range(1, n_tp):
        copy_w(k).wait_send()
        copy_m(k).wait_send()
    if part > 1:
        copy_r(lead).wait_send()
    for k in range(1, inner):
        copy_b1(k, here).wait_send()
        copy_f1(k, here).wait_send()
        for h in range(heads):
            copy_k(k, here, h).wait_send()
        copy_x(k).wait_send()
    each(outer - plane, outer, lambda k: copy_b2(k, plane).wait_send())
    each(1, outer - plane, lambda k: copy_f2(k, plane).wait_send())
    for k in range(1, outer):
        for h in range(heads):
            copy_p(k, h).wait_send()


def hand_on(*refs):
    copies = [
        pltpu.make_async_copy(refs[i], refs[4 + i], refs[8].at[i]) for i in range(4)
    ]
    for copy in copies:
        copy.start()
    for copy in copies:
        copy.wait()


def on_device(n, n_tp, block_input, value_weight, query_pre, forget_pre, lower_bound, out_grad):
    tokens, depth = block_input.shape
    width = query_pre.shape[1]
    heads = width // HEAD
    rows = depth // n
    inner = 1
    while n % (inner * 2) == 0 and (inner * 2) ** 2 <= n:
        inner *= 2
    outer = n // inner
    part = 2 if n_tp == 2 and rows % 32 == 0 else 1
    message = (heads // 2) * HEAD + (heads % 2) * HEAD // 2 + LOGROWS
    dma = pltpu.SemaphoreType.DMA
    vmem = pl.BlockSpec(memory_space=pltpu.VMEM)
    anywhere = pl.BlockSpec(memory_space=pl.ANY)
    results = pl.pallas_call(
        functools.partial(kernel, inner, outer, n_tp, part),
        out_shape=(
            pltpu.VMEM((width, tokens), bf16),
            pltpu.VMEM((width, tokens), bf16),
            pltpu.VMEM((tokens // n_tp, depth), bf16),
            pltpu.VMEM((width, rows), f32),
        ),
        in_specs=[anywhere] * 4 + [vmem, anywhere],
        out_specs=(vmem,) * 4,
        scratch_shapes=[
            pltpu.VMEM((tokens, depth), bf16),
            pltpu.VMEM((width, depth), bf16),
            pltpu.VMEM((width, tokens), bf16),
            pltpu.VMEM((width, tokens), bf16),
            pltpu.VMEM((width, tokens), bf16),
            dma((5,)),
            pltpu.VMEM((n_tp - 1, width, depth), bf16),
            pltpu.VMEM((outer, inner, part, rows // part, tokens), bf16),
            pltpu.VMEM((outer, part, rows // part, inner * tokens), bf16),
            pltpu.VMEM((inner, message, 2 * HEAD), bf16),
            pltpu.VMEM((inner, message, 2 * HEAD), bf16),
            pltpu.VMEM((message, 2 * HEAD), bf16),
            pltpu.VMEM((message, 2 * HEAD), bf16),
            pltpu.VMEM((outer, message, 2 * HEAD), bf16),
            pltpu.VMEM((outer, message, 2 * HEAD), bf16),
            pltpu.VMEM((inner, heads, 2, HEAD, tokens), bf16),
            pltpu.VMEM((width, inner * tokens), bf16),
            pltpu.VMEM((n_tp - 1, width, tokens), bf16),
            pltpu.VMEM((heads, outer, HEAD, rows), bf16),
            pltpu.VMEM((outer - 1, heads, HEAD, rows), bf16),
            pltpu.VMEM((n_tp, tokens, width), bf16),
            dma((n_tp - 1,)), dma((n_tp - 1,)),
            dma((inner - 1,)), dma((inner - 1,)),
            dma((1,)), dma((1,)),
            dma((inner - 1,)), dma((inner - 1,)),
            dma((inner - 1,)), dma((inner - 1,)),
            dma((outer - 1,)), dma((outer - 1,)),
            dma((outer - 1,)), dma((outer - 1,)),
            dma((heads * (inner - 1),)), dma((heads * (inner - 1),)),
            dma((n_tp - 1,)), dma((n_tp - 1,)),
            dma((heads * (outer - 1),)), dma((heads * (outer - 1),)),
        ],
        compiler_params=pltpu.CompilerParams(
            collective_id=0, has_side_effects=True, vmem_limit_bytes=60 * 1024 * 1024
        ),
    )(block_input, value_weight.T, query_pre.T, forget_pre.T, lower_bound[None, :], out_grad.T)
    gq, gf, gx, gw = pl.pallas_call(
        hand_on,
        out_shape=tuple(jax.ShapeDtypeStruct(a.shape, a.dtype) for a in results),
        in_specs=[vmem] * 4,
        out_specs=(anywhere,) * 4,
        scratch_shapes=[dma((4,))],
    )(*[pltpu.with_memory_space_constraint(a, pltpu.VMEM) for a in results])
    return gq.T, gf.T, gx, gw.T


def solution(mesh):
    n, n_tp = mesh.shape["sp"], mesh.shape["tp"]
    in_specs = (P("sp", None), P(None, "tp"), P("sp", "tp"), P("sp", "tp"), P("tp"), P("sp", "tp"))
    out_specs = (P("sp", "tp"), P("sp", "tp"), P(("sp", "tp"), None), P("sp", "tp"))
    return jax.shard_map(
        functools.partial(on_device, n, n_tp),
        mesh=mesh, in_specs=in_specs, out_specs=out_specs, check_vma=False,
    )
```

```python
import functools

import jax
import jax.numpy as jnp
from jax import lax
from jax.experimental import pallas as pl
from jax.experimental.pallas import tpu as pltpu
from jax.sharding import PartitionSpec as P

HEAD = 64
MESH = pl.DeviceIdType.MESH
f32, bf16 = jnp.float32, jnp.bfloat16
LOGROWS = 16


def nn(a, b):
    return lax.dot_general(a, b, (((1,), (0,)), ((), ())), preferred_element_type=f32)


def nt(a, b):
    return lax.dot_general(a, b, (((1,), (1,)), ((), ())), preferred_element_type=f32)


def tn(a, b):
    return lax.dot_general(a, b, (((0,), (0,)), ((), ())), preferred_element_type=f32)


def split(a):
    high = a.astype(bf16)
    return high, (a - high.astype(f32)).astype(bf16)


def kernel(
    inner, outer, n_tp, part,
    x_in, w_in, q_hbm, f_hbm, lb_ref, g_in,
    gq_ref, gf_ref, gx_ref, gw_ref,
    x_ref, w_ref, q_ref, f_ref, g_ref, in_sem,
    w_all, xt, xg, b1, f1, bmsg, fmsg, b2, f2, gvk, dvp, dvm, pmsg, pin, dvs,
    w_send, w_recv, x_send, x_recv, r_send, r_recv, b1_send, b1_recv, f1_send, f1_recv,
    b2_send, b2_recv, f2_send, f2_recv, k_send, k_recv, m_send, m_recv, p_send, p_recv,
):
    me, core = lax.axis_index("sp"), lax.axis_index("tp")
    here, plane = lax.rem(me, inner), me // inner
    tokens, depth = x_ref.shape
    width = q_ref.shape[0]
    heads = width // HEAD
    half = tokens // n_tp
    pairs, odd = heads // 2, heads % 2
    wide = 2 * HEAD
    packed = pairs * HEAD + odd * HEAD // 2

    def near(k):
        return (plane * inner + lax.rem(here + k, inner), core)

    def column(k):
        return (lax.rem(plane + k, outer) * inner + here, core)

    def mate(k):
        return (me, lax.rem(core + k, n_tp))

    def rc(src, dst, send, recv, k, to):
        return pltpu.make_async_remote_copy(src, dst, send.at[k - 1], recv.at[k - 1], to, MESH)

    loads = [
        pltpu.make_async_copy(src, dst, in_sem.at[i])
        for i, (src, dst) in enumerate(
            ((f_hbm, f_ref), (q_hbm, q_ref), (g_in, g_ref), (w_in, w_ref), (x_in, x_ref))
        )
    ]
    for load in loads:
        load.start()
    barrier = pltpu.get_barrier_semaphore()
    for to, count in ((near, inner), (column, outer), (mate, n_tp)):
        for k in range(1, count):
            pl.semaphore_signal(barrier, inc=1, device_id=to(k), device_id_type=MESH)

    lead = core * (part - 1)
    own_lanes = pl.ds(pl.multiple_of(here * tokens, tokens), tokens)

    def copy_w(k):
        return rc(w_ref, w_all.at[k - 1], w_send, w_recv, k, mate(k))

    def copy_x(k):
        return rc(
            xt.at[:, lax.rem(here + k, inner), lead], xg.at[:, lead, :, own_lanes],
            x_send, x_recv, k, near(k),
        )

    def copy_r(lane):
        return rc(xg.at[:, lane], xg.at[:, lane], r_send, r_recv, 1, mate(1))

    def copy_b1(k, at):
        return rc(b1.at[at], b1.at[at], b1_send, b1_recv, k, near(k))

    def copy_f1(k, at):
        return rc(f1.at[at], f1.at[at], f1_send, f1_recv, k, near(k))

    def copy_k(k, at, h):
        each_h = (inner - 1) * h + k
        return rc(gvk.at[at, h], gvk.at[at, h], k_send, k_recv, each_h, near(k))

    def copy_b2(k, at):
        return rc(bmsg, b2.at[at], b2_send, b2_recv, k, column(k))

    def copy_f2(k, at):
        return rc(fmsg, f2.at[at], f2_send, f2_recv, k, column(k))

    def copy_m(k):
        return rc(dvp.at[:, own_lanes], dvm.at[k - 1], m_send, m_recv, k, mate(k))

    def copy_p(k, h):
        return rc(
            pmsg.at[h, lax.rem(plane + k, outer)], pin.at[k - 1, h],
            p_send, p_recv, (outer - 1) * h + k, column(k),
        )

    def source(k):
        return lax.rem(here + inner - k, inner)

    lane_low = lax.broadcasted_iota(jnp.int32, (1, wide), 1) < HEAD

    def pairs_of(a, j):
        return a[j * wide : (j + 1) * wide, :]

    def twice(a):
        return jnp.concatenate([a[pairs * wide :, :]] * 2, axis=0)

    def pack(values, keys):
        out = []
        for j in range(pairs):
            full = nt(pairs_of(values, j), pairs_of(keys, j))
            out.append(jnp.where(lane_low, full[:HEAD, :], full[HEAD:, :]))
        if odd:
            full = nt(values[pairs * wide :, :], twice(keys))
            out.append(jnp.where(lane_low, full[: HEAD // 2, :], full[HEAD // 2 :, :]))
        return jnp.concatenate(out, axis=0)

    def opened(state):
        out = []
        for j in range(pairs + odd):
            size = HEAD if j < pairs else HEAD // 2
            rows_of = state[j * HEAD : j * HEAD + size, :]
            out.append(
                jnp.concatenate(
                    [jnp.where(lane_low, rows_of, 0.0), jnp.where(lane_low, 0.0, rows_of)], axis=0
                ).astype(bf16)
            )
        return out

    def from_values(blocks, a):
        out = [tn(blocks[j], pairs_of(a, j)) for j in range(pairs)]
        if odd:
            full = tn(blocks[pairs], a[pairs * wide :, :])
            out.append(full[:HEAD, :] + full[HEAD:, :])
        return jnp.concatenate(out, axis=0)

    def scaled(logs, state):
        out = []
        for j in range(pairs + odd):
            size = HEAD if j < pairs else HEAD // 2
            out.append(jnp.exp(logs[j]) * state[j * HEAD : j * HEAD + size, :])
        return jnp.concatenate(out, axis=0)

    row_at = lax.broadcasted_iota(jnp.int32, (LOGROWS, wide), 0)

    def log_rows(logs):
        rows_f = jnp.zeros((LOGROWS, wide), f32)
        for j, log in enumerate(logs):
            high, low = split(log)
            rows_f = jnp.where(row_at == 2 * j, high.astype(f32), rows_f)
            rows_f = jnp.where(row_at == 2 * j + 1, low.astype(f32), rows_f)
        return rows_f.astype(bf16)

    def read(ref, at):
        state = ref[at, 0:packed, :].astype(f32)
        tail = ref[at, packed : packed + LOGROWS, :].astype(f32)
        logs = [tail[2 * j : 2 * j + 1, :] + tail[2 * j + 1 : 2 * j + 2, :] for j in range(pairs + odd)]
        return state, logs

    def added(a, b):
        return [p + q for p, q in zip(a, b)]

    s_at = lax.broadcasted_iota(jnp.int32, (tokens, tokens), 0)
    t_at = lax.broadcasted_iota(jnp.int32, (tokens, tokens), 1)
    upper, lower = s_at <= t_at, s_at >= t_at
    upper_b, lower_b = upper.astype(f32).astype(bf16), lower.astype(f32).astype(bf16)
    ones = jnp.ones((LOGROWS, tokens), bf16)
    lb = jnp.broadcast_to(lb_ref[...], (tokens, width)).T
    loads[0].wait()
    f_in = f_ref[...].astype(f32)
    f_sig = jax.nn.sigmoid(f_in)
    key = (1.0 - lb) * jax.nn.sigmoid(-f_in)
    high, low = split(jnp.log1p(-key))
    cumulative = nn(high, upper_b) + nn(low, upper_b)
    growth = jnp.exp(cumulative)
    loads[1].wait()
    q_in = q_ref[...].astype(f32)
    q_sig = jax.nn.sigmoid(q_in)
    query = q_in * q_sig
    q_dec = (query * growth).astype(bf16)
    loads[2].wait()
    g = g_ref[...]
    logs = []
    for j in range(pairs):
        logs.append((nt(ones, pairs_of(high, j)) + nt(ones, pairs_of(low, j)))[0:1, :])
    if odd:
        logs.append((nt(ones, twice(high)) + nt(ones, twice(low)))[0:1, :])
    tail = log_rows(logs)
    b1[here, 0:packed, :] = pack(g, q_dec).astype(bf16)
    b1[here, packed : packed + LOGROWS, :] = tail
    pl.semaphore_wait(barrier, inner + outer + n_tp - 3)
    for k in range(1, inner):
        copy_b1(k, here).start()
    loads[3].wait()
    for k in range(1, n_tp):
        copy_w(k).start()
    loads[4].wait()
    xt[...] = x_ref[...].T.reshape(xt.shape)
    for k in range(1, inner):
        copy_x(k).start()
    xg[:, lead, :, own_lanes] = xt[:, here, lead]

    value = nt(w_ref[...], x_ref[...]).astype(bf16)
    closing = cumulative[:, tokens - 1 : tokens]
    k_end = (key * jnp.exp(closing - cumulative)).astype(bf16)
    update = pack(value, k_end)
    f1[here, 0:packed, :] = update.astype(bf16)
    f1[here, packed : packed + LOGROWS, :] = tail
    for k in range(1, inner):
        copy_f1(k, here).start()
    shrinking = jnp.exp(-cumulative)
    k_dec = (key * shrinking).astype(bf16)

    def of(a, h):
        return a[h * HEAD : (h + 1) * HEAD, :]

    for h in range(heads):
        mixing = jnp.where(upper, tn(of(k_dec, h), of(q_dec, h)), 0.0).astype(bf16)
        gvk[here, h, 0] = nt(of(g, h), mixing).astype(bf16)
        gvk[here, h, 1] = of(k_end, h)
        for k in range(1, inner):
            copy_k(k, here, h).start()

    for k in range(1, inner):
        copy_b1(k, source(k)).wait_recv()
    inside, after = [None] * inner, [None] * inner
    running = jnp.zeros((packed, wide), f32)
    plane_logs = [jnp.zeros((1, wide), f32) for _ in range(pairs + odd)]
    for j in reversed(range(inner)):
        inside[j], after[j] = running, plane_logs
        state, own_logs = read(b1, j)
        running = state + scaled(own_logs, running)
        plane_logs = added(plane_logs, own_logs)
    plane_tail = log_rows(plane_logs)
    bmsg[0:packed, :] = running.astype(bf16)
    bmsg[packed : packed + LOGROWS, :] = plane_tail

    def each(lo, hi, act):
        def step(i, carried):
            act(i)
            return carried

        lax.fori_loop(lo, hi, step, 0)

    each(outer - plane, outer, lambda k: copy_b2(k, plane).start())

    pairing = [jnp.where(upper, tn(of(value, h), of(g, h)), 0.0).astype(bf16) for h in range(heads)]
    gk_local = jnp.concatenate([nt(of(q_dec, h), pairing[h]) for h in range(heads)], axis=0)
    gq_local = jnp.concatenate([nn(of(k_dec, h), pairing[h]) for h in range(heads)], axis=0)

    for k in range(1, inner):
        lanes = pl.ds(pl.multiple_of(source(k) * tokens, tokens), tokens)
        rc(xt.at[:, 0, lead], xg.at[:, lead, :, lanes], x_send, x_recv, k, near(k)).wait_recv()
    if part > 1:
        copy_r(lead).start()

    for k in range(1, inner):
        copy_f1(k, source(k)).wait_recv()
    running = jnp.zeros((packed, wide), f32)
    before = [jnp.zeros((1, wide), f32) for _ in range(pairs + odd)]
    incoming = running
    in_logs = before
    for j in range(inner):
        incoming = jnp.where(here == j, running, incoming)
        in_logs = [jnp.where(here == j, p, q) for p, q in zip(before, in_logs)]
        state, own_logs = read(f1, j)
        running = state + scaled(own_logs, running)
        before = added(before, own_logs)
    fmsg[0:packed, :] = running.astype(bf16)
    fmsg[packed : packed + LOGROWS, :] = plane_tail
    each(1, outer - plane, lambda k: copy_f2(k, plane).start())

    empty = jnp.zeros((packed, wide), f32)
    none = [jnp.zeros((1, wide), f32) for _ in range(pairs + odd)]

    def entering(ref, copy, count, place, distance):
        def step(i, carried):
            total, weight = carried
            copy(distance(i), place(i)).wait_recv()
            state, own_logs = read(ref, place(i))
            return total + scaled(weight, state), added(weight, own_logs)

        return lax.fori_loop(0, count, step, (empty, none))[0]

    below = entering(
        b2, copy_b2, outer - 1 - plane, lambda i: plane + 1 + i, lambda i: outer - 1 - i
    )
    outgoing = empty
    opens = []
    for j in range(inner):
        grad_state = inside[j] + scaled(after[j], below)
        outgoing = jnp.where(here == j, grad_state, outgoing)
        opens.append(opened(grad_state))
    if part > 1:
        copy_r(1 - lead).wait_recv()
    for h in range(heads):
        for k in range(1, inner):
            copy_k(k, source(k), h).wait_recv()
        at = slice(h * HEAD, (h + 1) * HEAD)
        for j in range(inner):
            block = opens[j][h // 2][h % 2 * HEAD : (h % 2 + 1) * HEAD, :]
            doubled = jnp.concatenate([gvk[j, h, 1]] * 2, axis=0)
            value_grad = gvk[j, h, 0].astype(f32) + nn(block, doubled)
            dvp[at, j * tokens : (j + 1) * tokens] = value_grad.astype(bf16)
        for z in range(outer):
            pieces = [nt(dvp[at, :], xg[z, p]) for p in range(part)]
            pmsg[h, z] = jnp.concatenate(pieces, axis=1).astype(bf16)
        for k in reversed(range(1, outer)):
            copy_p(k, h).start()
    for k in range(1, n_tp):
        copy_m(k).start()

    def rows_half(a, slot):
        dvs[slot] = a.T
        return dvs[slot, pl.ds(pl.multiple_of(core * half, half), half), :]

    gx = nn(rows_half(dvp[:, own_lanes], 0), w_ref[...]).astype(bf16).astype(f32)
    for k in range(1, n_tp):
        copy_w(k).wait_recv()
        copy_m(k).wait_recv()
        gx = gx + nn(rows_half(dvm[k - 1], k), w_all[k - 1]).astype(bf16).astype(f32)
    gx_ref[...] = gx.astype(bf16)

    above = entering(f2, copy_f2, plane, lambda i: plane - 1 - i, lambda i: i + 1)
    incoming = incoming + scaled(in_logs, above)
    grad_query = growth * (gq_local + from_values(opened(incoming), g))
    remaining = jnp.exp(closing - cumulative)
    grad_key = shrinking * gk_local + remaining * from_values(opened(outgoing), value)
    product = outgoing * (scaled(logs, incoming) + update)
    p_high, p_low = split(product)
    bound = []
    for j in range(pairs + odd):
        size = HEAD if j < pairs else HEAD // 2
        every = jnp.ones((size, tokens), bf16)
        at = slice(j * HEAD, j * HEAD + size)
        full = tn(p_high[at, :], every) + tn(p_low[at, :], every)
        bound.append(full if j < pairs else full[:HEAD, :] + full[HEAD:, :])
    boundary = jnp.concatenate(bound, axis=0)
    c_high, c_low = split(query * grad_query - key * grad_key)
    grad_decay = nn(c_high, lower_b) + nn(c_low, lower_b) + boundary
    gq_ref[...] = (grad_query * (q_sig * (1.0 + q_in * (1.0 - q_sig)))).astype(bf16)
    gf_ref[...] = (-(grad_key - grad_decay / (1.0 - key)) * key * f_sig).astype(bf16)

    for h in range(heads):
        total = pmsg[h, plane].astype(f32)
        for k in range(1, outer):
            copy_p(k, h).wait_recv()
            total = total + pin[k - 1, h].astype(f32)
        gw_ref[h * HEAD : (h + 1) * HEAD, :] = total

    for k in range(1, n_tp):
        copy_w(k).wait_send()
        copy_m(k).wait_send()
    if part > 1:
        copy_r(lead).wait_send()
    for k in range(1, inner):
        copy_b1(k, here).wait_send()
        copy_f1(k, here).wait_send()
        for h in range(heads):
            copy_k(k, here, h).wait_send()
        copy_x(k).wait_send()
    each(outer - plane, outer, lambda k: copy_b2(k, plane).wait_send())
    each(1, outer - plane, lambda k: copy_f2(k, plane).wait_send())
    for k in range(1, outer):
        for h in range(heads):
            copy_p(k, h).wait_send()


def hand_on(*refs):
    copies = [
        pltpu.make_async_copy(refs[i], refs[4 + i], refs[8].at[i]) for i in range(4)
    ]
    for copy in copies:
        copy.start()
    for copy in copies:
        copy.wait()


def on_device(n, n_tp, block_input, value_weight, query_pre, forget_pre, lower_bound, out_grad):
    tokens, depth = block_input.shape
    width = query_pre.shape[1]
    heads = width // HEAD
    rows = depth // n
    inner = 1
    while n % (inner * 2) == 0 and (inner * 2) ** 2 <= n:
        inner *= 2
    outer = n // inner
    part = 2 if n_tp == 2 and rows % 32 == 0 else 1
    message = (heads // 2) * HEAD + (heads % 2) * HEAD // 2 + LOGROWS
    dma = pltpu.SemaphoreType.DMA
    vmem = pl.BlockSpec(memory_space=pltpu.VMEM)
    anywhere = pl.BlockSpec(memory_space=pl.ANY)
    results = pl.pallas_call(
        functools.partial(kernel, inner, outer, n_tp, part),
        out_shape=(
            pltpu.VMEM((width, tokens), bf16),
            pltpu.VMEM((width, tokens), bf16),
            pltpu.VMEM((tokens // n_tp, depth), bf16),
            pltpu.VMEM((width, rows), f32),
        ),
        in_specs=[anywhere] * 4 + [vmem, anywhere],
        out_specs=(vmem,) * 4,
        scratch_shapes=[
            pltpu.VMEM((tokens, depth), bf16),
            pltpu.VMEM((width, depth), bf16),
            pltpu.VMEM((width, tokens), bf16),
            pltpu.VMEM((width, tokens), bf16),
            pltpu.VMEM((width, tokens), bf16),
            dma((5,)),
            pltpu.VMEM((n_tp - 1, width, depth), bf16),
            pltpu.VMEM((outer, inner, part, rows // part, tokens), bf16),
            pltpu.VMEM((outer, part, rows // part, inner * tokens), bf16),
            pltpu.VMEM((inner, message, 2 * HEAD), bf16),
            pltpu.VMEM((inner, message, 2 * HEAD), bf16),
            pltpu.VMEM((message, 2 * HEAD), bf16),
            pltpu.VMEM((message, 2 * HEAD), bf16),
            pltpu.VMEM((outer, message, 2 * HEAD), bf16),
            pltpu.VMEM((outer, message, 2 * HEAD), bf16),
            pltpu.VMEM((inner, heads, 2, HEAD, tokens), bf16),
            pltpu.VMEM((width, inner * tokens), bf16),
            pltpu.VMEM((n_tp - 1, width, tokens), bf16),
            pltpu.VMEM((heads, outer, HEAD, rows), bf16),
            pltpu.VMEM((outer - 1, heads, HEAD, rows), bf16),
            pltpu.VMEM((n_tp, tokens, width), bf16),
            dma((n_tp - 1,)), dma((n_tp - 1,)),
            dma((inner - 1,)), dma((inner - 1,)),
            dma((1,)), dma((1,)),
            dma((inner - 1,)), dma((inner - 1,)),
            dma((inner - 1,)), dma((inner - 1,)),
            dma((outer - 1,)), dma((outer - 1,)),
            dma((outer - 1,)), dma((outer - 1,)),
            dma((heads * (inner - 1),)), dma((heads * (inner - 1),)),
            dma((n_tp - 1,)), dma((n_tp - 1,)),
            dma((heads * (outer - 1),)), dma((heads * (outer - 1),)),
        ],
        compiler_params=pltpu.CompilerParams(
            collective_id=0, has_side_effects=True, vmem_limit_bytes=60 * 1024 * 1024
        ),
    )(block_input, value_weight.T, query_pre.T, forget_pre.T, lower_bound[None, :], out_grad.T)
    gq, gf, gx, gw = pl.pallas_call(
        hand_on,
        out_shape=tuple(jax.ShapeDtypeStruct(a.shape, a.dtype) for a in results),
        in_specs=[vmem] * 4,
        out_specs=(anywhere,) * 4,
        scratch_shapes=[dma((4,))],
    )(*[pltpu.with_memory_space_constraint(a, pltpu.VMEM) for a in results])
    return gq.T, gf.T, gx, gw.T


def solution(mesh):
    n, n_tp = mesh.shape["sp"], mesh.shape["tp"]
    in_specs = (P("sp", None), P(None, "tp"), P("sp", "tp"), P("sp", "tp"), P("tp"), P("sp", "tp"))
    out_specs = (P("sp", "tp"), P("sp", "tp"), P(("sp", "tp"), None), P("sp", "tp"))
    return jax.shard_map(
        functools.partial(on_device, n, n_tp),
        mesh=mesh, in_specs=in_specs, out_specs=out_specs, check_vma=False,
    )
```
